512 devices in a mesh: sp: 64 (over z, y), tp: 8 (over x, core).
Axes of the slice: x: 4, y: 8, z: 8, core: 2. Of those that a mesh axis runs over, the one named last changes fastest.
Arguments:
- value_in: bfloat16 [23040, 2048], P('sp', 'tp'), may hold values from -240 to 240
- gate_in: bfloat16 [23040, 2048], P('sp', 'tp'), may hold values from -8 to 8
- taps: float32 [31, 2048], P(None, 'tp'), may hold values from -1 to 1
- norm_gain: float32 [2048], P('tp'), may hold values from 0.1 to 1.9
- norm_bias: float32 [2048], P('tp'), may hold values from -3 to 3
- proj_weight: bfloat16 [2048, 4096], P('tp', 'sp'), may hold values from -0.125 to 0.125
- out_grad: bfloat16 [23040, 4096], P('sp'), may hold values from -16 to 16
Outputs:
- value_grad: bfloat16 [23040, 2048], P('sp', 'tp')
- gate_grad: bfloat16 [23040, 2048], P('sp', 'tp')
- tap_grad: float32 [31, 2048], P(None, 'tp')
- gain_grad: float32 [2048], P('tp')
- bias_grad: float32 [2048], P('tp')
- weight_grad: float32 [2048, 4096], P('tp', 'sp')
The draws below stay inside these ranges and needn't reach their ends.
All inputs are finite; a program needn't handle non-finite values.
Results may differ from the reference program's by a relative error of at most 0.0051.
Values may be sent and summed in bfloat16 or wider, within the bound.
A program may use at most 64 MiB of HBM per device.

```python
import math
import jax
import jax.numpy as jnp
from jax import lax

MODEL = 4096
CHANNELS = 2048
TAPS = 31
TOKENS = 23040


def draw_value_in(key, part):
    first, second = jax.random.split(key, 2)
    chan = jnp.exp(jnp.linspace(0.0, math.log(10.0), CHANNELS)) * jax.random.uniform(second, (CHANNELS,), jnp.float32, 0.5, 2.0)
    along = jnp.exp(jnp.linspace(0.0, math.log(3.0), TOKENS))[:, None]
    base = jnp.clip(jax.random.normal(first, (TOKENS, CHANNELS), jnp.float32), -4.0, 4.0)
    return jnp.clip(base * chan[None, :] * along, -240.0, 240.0).astype(jnp.bfloat16)


def with_spikes(drawn, rng, source, target, blocks, factor):
    def block_of(position):
        return (jnp.arange(drawn.shape[position]) // (drawn.shape[position] // blocks)).reshape((-1,) + (1,) * (drawn.ndim - 1 - position))

    one_side = jax.random.permutation(rng, blocks)[block_of(target)]
    second = (block_of(target) + blocks // 2) % blocks
    return jnp.where((block_of(source) == one_side) | (block_of(source) == second), factor * drawn, drawn)


def levels(rng, shape, cuts, smallest, largest):
    loudness = 1.0
    for axis_at, shards_of in cuts:
        heights = jax.random.uniform(jax.random.fold_in(jax.random.fold_in(rng, 6), axis_at), (shards_of,), jnp.float32, smallest / len(cuts), largest / len(cuts))
        loudness = loudness * jnp.repeat(jnp.exp(heights), shape[axis_at] // shards_of).reshape((-1,) + (1,) * (len(shape) - 1 - axis_at))
    return loudness


def gaussian(key, dims, width, most, cuts=(), dtype=jnp.bfloat16):
    loudness = levels(key, dims, cuts, -0.22, 0.18) if cuts else 1.0
    values = jax.random.normal(key, dims, jnp.float32) * width * loudness
    return jnp.minimum(jnp.maximum(values, -most), most).astype(dtype)


def heavy_noise(stream_key, shape, scale, reach, cuts, heavy, kind=jnp.bfloat16):
    values = scale * jax.random.normal(stream_key, shape, jnp.float32)
    if cuts:
        values = values * levels(stream_key, shape, cuts, -0.22, 0.18)
    return jnp.clip(with_spikes(values, jax.random.fold_in(stream_key, 3), *heavy), -reach, reach).astype(kind)


def setup_inputs(seed: int = 0) -> dict:
    streams_of = jax.random.split(jax.random.key(seed), 8)
    return {
        "value_in": draw_value_in(jax.random.fold_in(streams_of[7], 71), 0),
        "gate_in": gaussian(streams_of[1], (TOKENS, CHANNELS), 2.0, 8.0, ((0, 64), (1, 8))),
        "taps": gaussian(streams_of[2], (TAPS, CHANNELS), TAPS ** -0.5, 1.0, ((1, 8),), jnp.float32),
        "norm_gain": jnp.clip(1.0 + 0.18 * jax.random.normal(streams_of[3], (CHANNELS,), jnp.float32), 0.1, 1.9),
        "norm_bias": gaussian(streams_of[4], (CHANNELS,), 0.5, 3.0, ((0, 8),), jnp.float32),
        "proj_weight": gaussian(streams_of[5], (CHANNELS, MODEL), CHANNELS ** -0.5, 0.125, ((0, 8), (1, 64))),
        "out_grad": heavy_noise(streams_of[6], (TOKENS, MODEL), 1.0, 16.0, ((0, 64),), (0, 1, 64, 4.0)),
    }


def reference(value_in, gate_in, taps, norm_gain, norm_bias, proj_weight, out_grad):
    f32 = jnp.float32
    rows = value_in.shape[0]
    span = taps.shape[0]
    half = span // 2
    width_all = value_in.shape[1]
    gate_sig = jax.nn.sigmoid(gate_in.astype(f32))
    value_f = value_in.astype(f32)
    mixed = (value_f * gate_sig).astype(jnp.bfloat16)
    padded = jnp.pad(mixed.astype(f32), ((half, half), (0, 0)))
    conv = jnp.zeros((rows, width_all), f32)
    for k in range(span):
        conv = conv + taps[k] * padded[k:k + rows]
    mean = lax.optimization_barrier(jnp.sum(conv, axis=1)) / width_all
    centred = conv - mean[:, None]
    spread = lax.optimization_barrier(jnp.sum(centred * centred, axis=1)) / width_all
    inv = lax.rsqrt(spread + 1e-06)
    normed = centred * inv[:, None]
    pre = normed * norm_gain + norm_bias
    act = jax.nn.silu(pre).astype(jnp.bfloat16)
    act_grad = lax.dot_general(out_grad, proj_weight, (((1,), (1,)), ((), ())), preferred_element_type=f32)
    weight_grad = lax.dot_general(act, out_grad, (((0,), (0,)), ((), ())), preferred_element_type=f32)
    sig_pre = jax.nn.sigmoid(pre)
    pre_grad = act_grad * sig_pre * (1.0 + pre * (1.0 - sig_pre))
    gain_grad = lax.optimization_barrier(jnp.sum(pre_grad * normed, axis=0))
    bias_grad = lax.optimization_barrier(jnp.sum(pre_grad, axis=0))
    normed_grad = pre_grad * norm_gain
    first = lax.optimization_barrier(jnp.sum(normed_grad, axis=1)) / width_all
    second = lax.optimization_barrier(jnp.sum(normed_grad * normed, axis=1)) / width_all
    conv_grad = inv[:, None] * (normed_grad - first[:, None] - normed * second[:, None])
    tap_grad = jnp.stack([lax.optimization_barrier(jnp.sum(conv_grad * padded[k:k + rows], axis=0)) for k in range(span)])
    grad_pad = jnp.pad(conv_grad, ((half, half), (0, 0)))
    mixed_grad = jnp.zeros((rows, width_all), f32)
    for k in range(span):
        mixed_grad = mixed_grad + taps[k] * grad_pad[2 * half - k:2 * half - k + rows]
    value_grad = (mixed_grad * gate_sig).astype(jnp.bfloat16)
    gate_grad = (mixed_grad * value_f * gate_sig * (1.0 - gate_sig)).astype(jnp.bfloat16)
    return (value_grad, gate_grad, tap_grad, gain_grad, bias_grad, weight_grad)
```

```python
import functools

import jax
import jax.numpy as jnp
from jax import lax
from jax.experimental import pallas as pl
from jax.experimental.pallas import tpu as pltpu
from jax.sharding import Mesh
from jax.sharding import PartitionSpec as P

SP = ("sp_0", "sp_1")
MESH = pl.DeviceIdType.MESH
EPS = 1e-06
F32 = jnp.float32
BF16 = jnp.bfloat16
EDGE = 16


def kernel(
    cfg,
    v_hbm,
    g_hbm,
    taps_ref,
    gain_ref,
    bias_ref,
    w_ref,
    og_hbm,
    vg_ref,
    gg_ref,
    small_ref,
    wg_ref,
    v_s,
    g_s,
    og_s,
    vf_s,
    sig_s,
    mpad,
    conv_s,
    s1_s,
    s2_s,
    b1_s,
    b2_s,
    ib_s,
    act_f,
    act_s,
    ag_s,
    cgpad,
    tacc,
    halo_send,
    halo_recv,
    cg_recv,
    st_send,
    st_recv,
    wt_s,
    wgt_s,
    rs_s,
    rs_r,
    q_s,
    q_r,
    ar_s,
    ar_r,
    local_sem,
    halo_ss,
    halo_rs,
    st_ss,
    st_rs,
    a1_ss,
    a1_rs,
    a2_ss,
    a2_rs,
    r1_ss,
    r1_rs,
    r2_ss,
    r2_rs,
    ar_ss,
    ar_rs,
):
    nz, ny, nt, rows, width, span, chunk = cfg
    z, y, t = lax.axis_index("sp_0"), lax.axis_index("sp_1"), lax.axis_index("tp")
    count = nz * ny
    s = z * ny + y
    lanes = width // 2
    channels = width * nt
    steps = rows // chunk
    padded_rows = s1_s.shape[0]
    quarter = w_ref.shape[1] // 2

    def at(zz, yy, tt):
        return (zz, yy, tt)

    def along(h, phase, shift):
        on_y = (h == 0) == (phase == 1)
        if on_y:
            return at(z, lax.rem(y + shift + ny, ny), t)
        return at(lax.rem(z + shift + nz, nz), y, t)

    def size(h, phase):
        return ny if (h == 0) == (phase == 1) else nz

    def place(h, phase):
        return y if (h == 0) == (phase == 1) else z

    def cell(h, a, b):
        return (b, a) if h == 0 else (a, b)

    pending = []

    def send(src, dst, ssem, rsem, dev):
        copy = pltpu.make_async_remote_copy(
            src_ref=src, dst_ref=dst, send_sem=ssem, recv_sem=rsem, device_id=dev, device_id_type=MESH
        )
        copy.start()
        pending.append(copy)
        return copy

    load_v = pltpu.make_async_copy(v_hbm, v_s, local_sem.at[0])
    load_g = pltpu.make_async_copy(g_hbm, g_s, local_sem.at[1])
    load_og = pltpu.make_async_copy(og_hbm, og_s, local_sem.at[2])
    load_g.start()
    load_v.start()
    load_og.start()

    right = lax.rem(s + 1, count)
    left = lax.rem(s + count - 1, count)
    right_dev = at(right // ny, lax.rem(right, ny), t)
    left_dev = at(left // ny, lax.rem(left, ny), t)
    barrier = pltpu.get_barrier_semaphore()
    peers = [right_dev, left_dev]
    peers += [at(z, lax.rem(y + d, ny), t) for d in range(1, ny)]
    peers += [at(lax.rem(z + d, nz), y, t) for d in range(1, nz)]
    peers += [at(z, y, lax.rem(t + d, nt)) for d in range(1, nt)]
    for dev in peers:
        pl.semaphore_signal(barrier, inc=1, device_id=dev, device_id_type=MESH)

    n_col = w_ref.shape[1]
    eye = jnp.where(
        lax.broadcasted_iota(jnp.int32, (n_col, n_col), 0) == lax.broadcasted_iota(jnp.int32, (n_col, n_col), 1),
        jnp.ones((n_col, n_col), F32),
        jnp.zeros((n_col, n_col), F32),
    ).astype(BF16)
    turned = lax.dot_general(eye, w_ref[...], (((1,), (1,)), ((), ())), preferred_element_type=F32)
    wt_s[z, y] = turned.astype(BF16).reshape(2, quarter, width)

    load_g.wait()
    load_v.wait()
    sig = jax.nn.sigmoid(g_s[...].astype(F32))
    sig_s[...] = sig
    vf = v_s[...].astype(F32)
    vf_s[...] = vf
    mixed = (vf * sig).astype(BF16)
    halo_send[0] = mixed[rows - EDGE :]
    halo_send[1] = mixed[:EDGE]
    mpad[EDGE : EDGE + rows] = mixed.astype(F32)

    pl.semaphore_wait(barrier, len(peers))

    halo = [
        send(halo_send.at[0], halo_recv.at[0], halo_ss.at[0], halo_rs.at[0], right_dev),
        send(halo_send.at[1], halo_recv.at[1], halo_ss.at[1], halo_rs.at[1], left_dev),
    ]

    first, ring = {}, {}

    def near(d, n):
        return min(d, n - d)

    def ring_depth(h, d, sign):
        n = size(h, 2)
        even = d % 2 == 0
        return n // 2 if even == (sign > 0) else n // 2 - 1

    def forward(h, d, sign, k):
        a = lax.rem(place(h, 1) - d + size(h, 1), size(h, 1))
        n = size(h, 2)
        b = lax.rem(place(h, 2) - sign * (k - 1) + n, n)
        block = wt_s.at[(*cell(h, a, b), h)]
        i = 0 if sign > 0 else 1
        ring[h, d, sign, k] = send(
            block, block, a2_ss.at[h, d, i, k - 1], a2_rs.at[h, d, i, k - 1], along(h, 2, sign)
        )

    def gather_start():
        for h in range(2):
            for sign in (1, -1):
                if ring_depth(h, 0, sign) >= 1:
                    forward(h, 0, sign, 1)
        for h in range(2):
            n = size(h, 1)
            block = wt_s.at[(*cell(h, place(h, 1), place(h, 2)), h)]
            for d in sorted(range(1, n), key=lambda d: near(d, n)):
                first[h, d] = send(block, block, a1_ss.at[h, d], a1_rs.at[h, d], along(h, 1, d))

    def gather_round(r):
        for h in range(2):
            n = size(h, 1)
            for d in sorted(range(n), key=lambda d: near(d, n)):
                k = r - near(d, n) + 1
                if (d == 0 and k == 1) or k < 1 or k > size(h, 2) // 2 + 1:
                    continue
                if k == 1:
                    first[h, d].wait_recv()
                for sign in (1, -1):
                    depth = ring_depth(h, d, sign)
                    if 1 <= k - 1 <= depth:
                        ring[h, d, sign, k - 1].wait_recv()
                    if k <= depth:
                        forward(h, d, sign, k)

    rounds = max(size(h, 1) // 2 + size(h, 2) // 2 + 1 for h in range(2))
    gather_start()

    halo[0].wait_recv()
    halo[1].wait_recv()
    mpad[:EDGE] = jnp.where(s == 0, 0.0, halo_recv[0].astype(F32))
    mpad[EDGE + rows :] = jnp.where(s == count - 1, 0.0, halo_recv[1].astype(F32))

    def fold(x):
        return x[:, :lanes] + x[:, lanes:]

    def wide(x):
        return jnp.concatenate([x, x], axis=1)

    def conv_step(i, carry):
        base = i * chunk
        total = jnp.zeros((chunk, width), F32)
        for k in range(span):
            total = total + taps_ref[k : k + 1, :] * mpad[pl.ds(base + k + 1, chunk), :]
        conv_s[pl.ds(base, chunk), :] = total
        s1_s[pl.ds(base, chunk), :] = fold(total)
        s2_s[pl.ds(base, chunk), :] = fold(total * total)
        return carry

    for i in range(steps):
        conv_step(i, 0)

    def row_sums(which):
        a = jnp.sum(jnp.transpose(s1_s[...]), axis=0, keepdims=True)
        b = jnp.sum(jnp.transpose(s2_s[...]), axis=0, keepdims=True)
        both = jnp.concatenate([a, b], axis=0)
        st_send[which] = both
        copies = []
        for d in range(1, nt):
            copies.append(
                send(
                    st_send.at[which],
                    st_recv.at[which, d],
                    st_ss.at[which, d],
                    st_rs.at[which, d],
                    at(z, y, lax.rem(t + d, nt)),
                )
            )
        return copies

    def gathered_sums(which, copies):
        total = st_send[which]
        for d in range(1, nt):
            copies[d - 1].wait_recv()
            total = total + st_recv[which, d]
        return total / channels

    def down_rows(row):
        return jnp.transpose(jnp.broadcast_to(row, (lanes, padded_rows)))

    sums = row_sums(0)
    gather_round(0)
    gather_round(1)
    total = gathered_sums(0, sums)
    mean = total[0:1]
    inv = lax.rsqrt(total[1:2] - mean * mean + EPS)
    b1_s[...] = down_rows(mean)
    ib_s[...] = down_rows(inv)

    def act_step(i, carry):
        here = pl.ds(pl.multiple_of(i * chunk, 8), chunk)
        normed = (conv_s[here, :] - wide(b1_s[here, :])) * wide(ib_s[here, :])
        conv_s[here, :] = normed
        pre = normed * gain_ref[...] + bias_ref[...]
        act_f[here, :] = pre * jax.nn.sigmoid(pre)
        return carry

    lax.fori_loop(0, steps, act_step, 0)
    act_s[...] = act_f[...].astype(BF16)
    load_og.wait()
    gather_round(2)

    block_cols = ny * n_col

    def grad_step(i, carry):
        columns = pl.ds(pl.multiple_of(i * block_cols, 128), block_cols)
        part = lax.dot_general(
            og_s[:, columns], act_s[...], (((0,), (0,)), ((), ())), preferred_element_type=F32
        )
        wgt_s[i] = part.reshape(ny, 2, quarter, width)
        return carry

    lax.fori_loop(0, nz, grad_step, 0)

    hops, last = {}, {}

    def piece(h, c, p):
        n = size(h, 1) // 2
        if h == 0:
            return wgt_s[p, c * n : (c + 1) * n, 0]
        return wgt_s[c * n : (c + 1) * n, p, 1]

    def reduce_depth(h, c, sign):
        n = size(h, 2)
        return n // 2 if (c == 0) == (sign > 0) else n // 2 - 1

    def reduce_round(j):
        for h in range(2):
            n = size(h, 2)
            part = pl.ds(0, size(h, 1) // 2)
            for c in range(2):
                for i, sign in enumerate((1, -1)):
                    depth = reduce_depth(h, c, sign)
                    k = j - (n // 2 - depth)
                    if k < 1 or k > depth:
                        continue
                    dest = lax.rem(place(h, 2) + sign * (depth - k + 1) + n, n)
                    value = piece(h, c, dest)
                    if k > 1:
                        hops[h, c, sign, k - 1].wait_recv()
                        value = value + rs_r[h, c, i, k - 2, part].astype(F32)
                    rs_s[h, c, i, k - 1, part] = value.astype(BF16)
                    hops[h, c, sign, k] = send(
                        rs_s.at[h, c, i, k - 1, part],
                        rs_r.at[h, c, i, k - 1, part],
                        r1_ss.at[h, c, i, k - 1],
                        r1_rs.at[h, c, i, k - 1],
                        along(h, 2, sign),
                    )

    def reduce_finish():
        for h in range(2):
            n = size(h, 1) // 2
            for c in range(2):
                value = piece(h, c, place(h, 2))
                for i, sign in enumerate((1, -1)):
                    depth = reduce_depth(h, c, sign)
                    if depth:
                        hops[h, c, sign, depth].wait_recv()
                        value = value + rs_r[h, c, i, depth - 1, pl.ds(0, n)].astype(F32)
                if h == 0:
                    wgt_s[place(h, 2), c * n : (c + 1) * n, 0] = value
                else:
                    wgt_s[c * n : (c + 1) * n, place(h, 2), 1] = value
                q_s[h, c * n : (c + 1) * n] = value.astype(BF16)
            n = size(h, 1)
            for d in sorted(range(1, n), key=lambda d: near(d, n)):
                to = lax.rem(place(h, 1) + d, n)
                last[h, d] = send(
                    q_s.at[h, to], q_r.at[h, d], r2_ss.at[h, d], r2_rs.at[h, d], along(h, 1, d)
                )

    def reduce_end():
        for h in range(2):
            value = wgt_s[z, y, h]
            for d in range(1, size(h, 1)):
                last[h, d].wait_recv()
                value = value + q_r[h, d].astype(F32)
            wg_ref[h] = value

    gather_round(3)
    reduce_round(1)
    for r in range(4, rounds):
        gather_round(r)
    reduce_round(2)

    def product_step(i, carry):
        columns = pl.ds(pl.multiple_of(i * block_cols, 128), block_cols)
        part = jnp.dot(
            og_s[:, columns], wt_s[i].reshape(block_cols, width), preferred_element_type=F32
        )
        ag_s[...] = ag_s[...] + part
        return carry

    ag_s[...] = jnp.zeros_like(ag_s)
    lax.fori_loop(0, nz, product_step, 0)
    reduce_round(3)

    def pre_step(i, carry):
        gain_sum, bias_sum = carry
        here = pl.ds(pl.multiple_of(i * chunk, 8), chunk)
        normed = conv_s[here, :]
        pre = normed * gain_ref[...] + bias_ref[...]
        gate = jax.nn.sigmoid(pre)
        pre_grad = ag_s[here, :] * gate * (1.0 + pre * (1.0 - gate))
        gain_sum = gain_sum + jnp.sum((pre_grad * normed).reshape(chunk // 8, 8, width), axis=0)
        bias_sum = bias_sum + jnp.sum(pre_grad.reshape(chunk // 8, 8, width), axis=0)
        normed_grad = pre_grad * gain_ref[...]
        ag_s[here, :] = normed_grad
        s1_s[here, :] = fold(normed_grad)
        s2_s[here, :] = fold(normed_grad * normed)
        return gain_sum, bias_sum

    none = jnp.zeros((8, width), F32)
    gain_sum, bias_sum = lax.fori_loop(0, steps, pre_step, (none, none))
    gain_row = jnp.sum(gain_sum, axis=0, keepdims=True)
    bias_row = jnp.sum(bias_sum, axis=0, keepdims=True)
    sums = row_sums(1)
    reduce_round(4)
    total = gathered_sums(1, sums)
    b1_s[...] = down_rows(total[0:1])
    b2_s[...] = down_rows(total[1:2])

    def conv_grad_step(i, carry):
        base = pl.multiple_of(i * chunk, 8)
        here = pl.ds(base, chunk)
        value = wide(ib_s[here, :]) * (
            ag_s[here, :] - wide(b1_s[here, :]) - conv_s[here, :] * wide(b2_s[here, :])
        )
        cgpad[pl.ds(pl.multiple_of(base + EDGE, 8), chunk), :] = value
        return carry

    lax.fori_loop(0, steps, conv_grad_step, 0)
    back = [
        send(cgpad.at[pl.ds(rows, EDGE)], cg_recv.at[0], halo_ss.at[2], halo_rs.at[2], right_dev),
        send(cgpad.at[pl.ds(EDGE, EDGE)], cg_recv.at[1], halo_ss.at[3], halo_rs.at[3], left_dev),
    ]

    tacc[...] = jnp.zeros_like(tacc)

    def tap_step(i, carry):
        base = i * chunk
        value = cgpad[pl.ds(base + EDGE, chunk), :]
        for k in range(span):
            term = value * mpad[pl.ds(base + k + 1, chunk), :]
            tacc[k] = tacc[k] + jnp.sum(term.reshape(chunk // 8, 8, width), axis=0)
        return carry

    for i in range(steps):
        tap_step(i, 0)
    own_small = jnp.concatenate(
        [jnp.sum(tacc[...], axis=1), gain_row, bias_row, jnp.zeros((small_ref.shape[0] - span - 2, width), F32)],
        axis=0,
    )
    small_ref[...] = own_small

    def small_send(phase):
        copies = {}
        for h in range(2):
            ar_s[phase - 1, h] = small_ref[:, h * lanes : (h + 1) * lanes].astype(BF16)
        for h in range(2):
            n = size(h, phase)
            for d in sorted(range(1, n), key=lambda d: near(d, n)):
                copies[h, d] = send(
                    ar_s.at[phase - 1, h],
                    ar_r.at[phase - 1, h, d],
                    ar_ss.at[phase - 1, h, d],
                    ar_rs.at[phase - 1, h, d],
                    along(h, phase, d),
                )
        return copies

    def small_add(phase, copies):
        for h in range(2):
            value = ar_s[phase - 1, h].astype(F32)
            for d in range(1, size(h, phase)):
                copies[h, d].wait_recv()
                value = value + ar_r[phase - 1, h, d].astype(F32)
            small_ref[:, h * lanes : (h + 1) * lanes] = value

    small_1 = small_send(1)
    reduce_finish()

    back[0].wait_recv()
    back[1].wait_recv()
    cgpad[:EDGE] = jnp.where(s == 0, 0.0, cg_recv[0])
    cgpad[EDGE + rows :] = jnp.where(s == count - 1, 0.0, cg_recv[1])

    def mixed_step(i, carry):
        base = i * chunk
        total = jnp.zeros((chunk, width), F32)
        for k in range(span):
            total = total + taps_ref[k : k + 1, :] * cgpad[pl.ds(base + span - k, chunk), :]
        ag_s[pl.ds(base, chunk), :] = total
        return carry

    for i in range(steps):
        mixed_step(i, 0)
    small_add(1, small_1)
    small_2 = small_send(2)
    scaled = ag_s[...] * sig_s[...]
    vg_ref[...] = scaled.astype(BF16)
    gg_ref[...] = (scaled * vf_s[...] * (1.0 - sig_s[...])).astype(BF16)
    reduce_end()
    small_add(2, small_2)
    for copy in pending:
        copy.wait_send()


def on_device(sizes, value_in, gate_in, taps, norm_gain, norm_bias, proj_weight, out_grad):
    nz, ny, nt = sizes
    rows, width = value_in.shape
    span = taps.shape[0]
    n_col = proj_weight.shape[1]
    quarter = n_col // 2
    columns = out_grad.shape[1]
    lanes = width // 2
    chunk = next(c for c in (72, 24, 8) if rows % c == 0)
    padded_rows = (rows + 127) // 128 * 128
    small_rows = (span + 2 + 15) // 16 * 16
    n_max = max(nz, ny)
    n_half = n_max // 2
    dma = pltpu.SemaphoreType.DMA
    vmem = pl.BlockSpec(memory_space=pltpu.VMEM)
    anywhere = pl.BlockSpec(memory_space=pl.ANY)
    cfg = (nz, ny, nt, rows, width, span, chunk)
    vg, gg, small, wg = pl.pallas_call(
        functools.partial(kernel, cfg),
        out_shape=(
            jax.ShapeDtypeStruct((rows, width), BF16),
            jax.ShapeDtypeStruct((rows, width), BF16),
            jax.ShapeDtypeStruct((small_rows, width), F32),
            jax.ShapeDtypeStruct((2, quarter, width), F32),
        ),
        in_specs=[anywhere, anywhere, vmem, vmem, vmem, vmem, anywhere],
        out_specs=(vmem, vmem, vmem, vmem),
        scratch_shapes=[
            pltpu.VMEM((rows, width), BF16),
            pltpu.VMEM((rows, width), BF16),
            pltpu.VMEM((rows, columns), BF16),
            pltpu.VMEM((rows, width), F32),
            pltpu.VMEM((rows, width), F32),
            pltpu.VMEM((rows + 2 * EDGE, width), F32),
            pltpu.VMEM((rows, width), F32),
            pltpu.VMEM((padded_rows, lanes), F32),
            pltpu.VMEM((padded_rows, lanes), F32),
            pltpu.VMEM((padded_rows, lanes), F32),
            pltpu.VMEM((padded_rows, lanes), F32),
            pltpu.VMEM((padded_rows, lanes), F32),
            pltpu.VMEM((rows, width), F32),
            pltpu.VMEM((rows, width), BF16),
            pltpu.VMEM((rows, width), F32),
            pltpu.VMEM((rows + 2 * EDGE, width), F32),
            pltpu.VMEM((span, 8, width), F32),
            pltpu.VMEM((2, EDGE, width), BF16),
            pltpu.VMEM((2, EDGE, width), BF16),
            pltpu.VMEM((2, EDGE, width), F32),
            pltpu.VMEM((2, 2, padded_rows), F32),
            pltpu.VMEM((2, nt, 2, padded_rows), F32),
            pltpu.VMEM((nz, ny, 2, quarter, width), BF16),
            pltpu.VMEM((nz, ny, 2, quarter, width), F32),
            pltpu.VMEM((2, 2, 2, n_half, n_half, quarter, width), BF16),
            pltpu.VMEM((2, 2, 2, n_half, n_half, quarter, width), BF16),
            pltpu.VMEM((2, n_max, quarter, width), BF16),
            pltpu.VMEM((2, n_max, quarter, width), BF16),
            pltpu.VMEM((2, 2, small_rows, lanes), BF16),
            pltpu.VMEM((2, 2, n_max, small_rows, lanes), BF16),
            dma((3,)),
            dma((4,)),
            dma((4,)),
            dma((2, nt)),
            dma((2, nt)),
            dma((2, n_max)),
            dma((2, n_max)),
            dma((2, n_max, 2, n_half)),
            dma((2, n_max, 2, n_half)),
            dma((2, 2, 2, n_half)),
            dma((2, 2, 2, n_half)),
            dma((2, n_max)),
            dma((2, n_max)),
            dma((2, 2, n_max)),
            dma((2, 2, n_max)),
        ],
        compiler_params=pltpu.CompilerParams(
            collective_id=0, has_side_effects=True, vmem_limit_bytes=60 * 1024 * 1024
        ),
        name="step",
    )(value_in, gate_in, taps, norm_gain[None, :], norm_bias[None, :], proj_weight, out_grad)
    weight_grad = jnp.transpose(wg.reshape(n_col, width))
    return (vg, gg, small[:span], small[span], small[span + 1], weight_grad)


def solution(mesh):
    tp = mesh.shape["tp"]
    ny = 8 if mesh.shape["sp"] % 8 == 0 else 2
    nz = mesh.shape["sp"] // ny
    finer = Mesh(mesh.devices.reshape(nz, ny, tp), (*SP, "tp"))
    in_specs = (P(SP, "tp"), P(SP, "tp"), P(None, "tp"), P("tp"), P("tp"), P("tp", SP), P(SP, None))
    out_specs = (P(SP, "tp"), P(SP, "tp"), P(None, "tp"), P("tp"), P("tp"), P("tp", SP))
    return jax.shard_map(
        functools.partial(on_device, (nz, ny, tp)),
        mesh=finer,
        in_specs=in_specs,
        out_specs=out_specs,
        check_vma=False,
    )
```

```python
import functools

import jax
import jax.numpy as jnp
from jax import lax
from jax.experimental import pallas as pl
from jax.experimental.pallas import tpu as pltpu
from jax.sharding import Mesh
from jax.sharding import PartitionSpec as P

SP = ("sp_0", "sp_1")
MESH = pl.DeviceIdType.MESH
EPS = 1e-06
F32 = jnp.float32
BF16 = jnp.bfloat16
EDGE = 16


def kernel(
    cfg,
    v_hbm,
    g_hbm,
    taps_hbm,
    gain_hbm,
    bias_hbm,
    w_hbm,
    og_hbm,
    vg_ref,
    gg_ref,
    small_ref,
    wg_ref,
    v_s,
    g_s,
    og_s,
    taps_ref,
    gain_ref,
    bias_ref,
    vf_s,
    sig_s,
    mpad,
    conv_s,
    s1_s,
    s2_s,
    b1_s,
    b2_s,
    ib_s,
    act_f,
    act_s,
    ag_s,
    cgpad,
    tacc,
    halo_send,
    halo_recv,
    cg_recv,
    st_send,
    st_recv,
    wt_s,
    wgt_s,
    rs_s,
    rs_r,
    q_s,
    q_r,
    ar_s,
    ar_r,
    local_sem,
    halo_ss,
    halo_rs,
    st_ss,
    st_rs,
    a1_ss,
    a1_rs,
    a2_ss,
    a2_rs,
    r1_ss,
    r1_rs,
    r2_ss,
    r2_rs,
    ar_ss,
    ar_rs,
):
    nz, ny, nt, rows, width, span, chunk = cfg
    z, y, t = lax.axis_index("sp_0"), lax.axis_index("sp_1"), lax.axis_index("tp")
    count = nz * ny
    s = z * ny + y
    lanes = width // 2
    channels = width * nt
    steps = rows // chunk
    padded_rows = s1_s.shape[0]
    quarter = w_hbm.shape[1]
    n_col = 2 * quarter

    def at(zz, yy, tt):
        return (zz, yy, tt)

    def along(h, phase, shift):
        on_y = (h == 0) == (phase == 1)
        if on_y:
            return at(z, lax.rem(y + shift + ny, ny), t)
        return at(lax.rem(z + shift + nz, nz), y, t)

    def size(h, phase):
        return ny if (h == 0) == (phase == 1) else nz

    def place(h, phase):
        return y if (h == 0) == (phase == 1) else z

    def cell(h, a, b):
        return (b, a) if h == 0 else (a, b)

    pending = []

    def send(src, dst, ssem, rsem, dev):
        copy = pltpu.make_async_remote_copy(
            src_ref=src, dst_ref=dst, send_sem=ssem, recv_sem=rsem, device_id=dev, device_id_type=MESH
        )
        copy.start()
        pending.append(copy)
        return copy

    load_v = pltpu.make_async_copy(v_hbm, v_s, local_sem.at[0])
    load_g = pltpu.make_async_copy(g_hbm, g_s, local_sem.at[1])
    load_og = pltpu.make_async_copy(og_hbm, og_s, local_sem.at[2])
    load_w = pltpu.make_async_copy(w_hbm, wt_s.at[z, y], local_sem.at[3])
    load_taps = pltpu.make_async_copy(taps_hbm, taps_ref, local_sem.at[4])
    load_gain = pltpu.make_async_copy(gain_hbm, gain_ref, local_sem.at[5])
    load_bias = pltpu.make_async_copy(bias_hbm, bias_ref, local_sem.at[6])
    for load in (load_g, load_v, load_w, load_taps, load_gain, load_bias, load_og):
        load.start()

    right = lax.rem(s + 1, count)
    left = lax.rem(s + count - 1, count)
    right_dev = at(right // ny, lax.rem(right, ny), t)
    left_dev = at(left // ny, lax.rem(left, ny), t)
    barrier = pltpu.get_barrier_semaphore()
    peers = [right_dev, left_dev]
    peers += [at(z, lax.rem(y + d, ny), t) for d in range(1, ny)]
    peers += [at(lax.rem(z + d, nz), y, t) for d in range(1, nz)]
    peers += [at(z, y, lax.rem(t + d, nt)) for d in range(1, nt)]
    for dev in peers:
        pl.semaphore_signal(barrier, inc=1, device_id=dev, device_id_type=MESH)

    load_g.wait()
    load_v.wait()
    sig = jax.nn.sigmoid(g_s[...].astype(F32))
    sig_s[...] = sig
    vf = v_s[...].astype(F32)
    vf_s[...] = vf
    mixed = (vf * sig).astype(BF16)
    halo_send[0] = mixed[rows - EDGE :]
    halo_send[1] = mixed[:EDGE]
    mpad[EDGE : EDGE + rows] = mixed.astype(F32)

    for load in (load_w, load_taps, load_gain, load_bias):
        load.wait()
    pl.semaphore_wait(barrier, len(peers))

    halo = [
        send(halo_send.at[0], halo_recv.at[0], halo_ss.at[0], halo_rs.at[0], right_dev),
        send(halo_send.at[1], halo_recv.at[1], halo_ss.at[1], halo_rs.at[1], left_dev),
    ]

    first, ring = {}, {}

    def near(d, n):
        return min(d, n - d)

    def ring_depth(h, d, sign):
        n = size(h, 2)
        even = d % 2 == 0
        return n // 2 if even == (sign > 0) else n // 2 - 1

    def forward(h, d, sign, k):
        a = lax.rem(place(h, 1) - d + size(h, 1), size(h, 1))
        n = size(h, 2)
        b = lax.rem(place(h, 2) - sign * (k - 1) + n, n)
        block = wt_s.at[(*cell(h, a, b), h)]
        i = 0 if sign > 0 else 1
        ring[h, d, sign, k] = send(
            block, block, a2_ss.at[h, d, i, k - 1], a2_rs.at[h, d, i, k - 1], along(h, 2, sign)
        )

    def gather_start():
        for h in range(2):
            for sign in (1, -1):
                if ring_depth(h, 0, sign) >= 1:
                    forward(h, 0, sign, 1)
        todo = [(near(d, size(h, 1)), d, h) for h in range(2) for d in range(1, size(h, 1))]
        for _, d, h in sorted(todo):
            block = wt_s.at[(*cell(h, place(h, 1), place(h, 2)), h)]
            first[h, d] = send(block, block, a1_ss.at[h, d], a1_rs.at[h, d], along(h, 1, d))

    def gather_round(r):
        todo = []
        for h in range(2):
            n = size(h, 1)
            for d in range(n):
                k = r - min(near(d, n), 2) + 1
                if (d == 0 and k == 1) or k < 1 or k > size(h, 2) // 2 + 1:
                    continue
                todo.append((near(d, n), d, h, k))
        for _, d, h, k in sorted(todo):
            if k == 1:
                first[h, d].wait_recv()
            for sign in (1, -1):
                depth = ring_depth(h, d, sign)
                if 1 <= k - 1 <= depth:
                    ring[h, d, sign, k - 1].wait_recv()
                if k <= depth:
                    forward(h, d, sign, k)

    rounds = max(min(size(h, 1) // 2, 2) + size(h, 2) // 2 + 1 for h in range(2))
    gather_start()

    halo[0].wait_recv()
    halo[1].wait_recv()
    mpad[:EDGE] = jnp.where(s == 0, 0.0, halo_recv[0].astype(F32))
    mpad[EDGE + rows :] = jnp.where(s == count - 1, 0.0, halo_recv[1].astype(F32))

    def fold(x):
        return x[:, :lanes] + x[:, lanes:]

    def wide(x):
        return jnp.concatenate([x, x], axis=1)

    def conv_step(i, carry):
        base = i * chunk
        total = jnp.zeros((chunk, width), F32)
        for k in range(span):
            total = total + taps_ref[k : k + 1, :] * mpad[pl.ds(base + k + 1, chunk), :]
        conv_s[pl.ds(base, chunk), :] = total
        s1_s[pl.ds(base, chunk), :] = fold(total)
        s2_s[pl.ds(base, chunk), :] = fold(total * total)
        return carry

    for i in range(2 * steps // 5):
        conv_step(i, 0)
    gather_round(1)
    for i in range(2 * steps // 5, steps):
        conv_step(i, 0)

    def row_sums(which):
        a = jnp.sum(jnp.transpose(s1_s[...]), axis=0, keepdims=True)
        b = jnp.sum(jnp.transpose(s2_s[...]), axis=0, keepdims=True)
        both = jnp.concatenate([a, b], axis=0)
        st_send[which] = both
        copies = []
        for d in range(1, nt):
            copies.append(
                send(
                    st_send.at[which],
                    st_recv.at[which, d],
                    st_ss.at[which, d],
                    st_rs.at[which, d],
                    at(z, y, lax.rem(t + d, nt)),
                )
            )
        return copies

    def gathered_sums(which, copies):
        total = st_send[which]
        for d in range(1, nt):
            copies[d - 1].wait_recv()
            total = total + st_recv[which, d]
        return total / channels

    def down_rows(row):
        return jnp.transpose(jnp.broadcast_to(row, (lanes, padded_rows)))

    sums = row_sums(0)
    gather_round(2)
    total = gathered_sums(0, sums)
    mean = total[0:1]
    inv = lax.rsqrt(total[1:2] - mean * mean + EPS)
    b1_s[...] = down_rows(mean)
    ib_s[...] = down_rows(inv)

    def act_step(i, carry):
        here = pl.ds(pl.multiple_of(i * chunk, 8), chunk)
        normed = (conv_s[here, :] - wide(b1_s[here, :])) * wide(ib_s[here, :])
        conv_s[here, :] = normed
        pre = normed * gain_ref[...] + bias_ref[...]
        act_f[here, :] = pre * jax.nn.sigmoid(pre)
        return carry

    lax.fori_loop(0, steps, act_step, 0)
    act_s[...] = act_f[...].astype(BF16)
    load_og.wait()
    gather_round(3)

    block_cols = ny * n_col

    def grad_step(i, carry):
        columns = pl.ds(pl.multiple_of(i * block_cols, 128), block_cols)
        part = lax.dot_general(
            og_s[:, columns], act_s[...], (((0,), (0,)), ((), ())), preferred_element_type=F32
        )
        wgt_s[i] = part.reshape(ny, 2, quarter, width)
        return carry

    lax.fori_loop(0, nz // 2, grad_step, 0)
    gather_round(4)
    lax.fori_loop(nz // 2, nz, grad_step, 0)

    hops, last = {}, {}

    def parts(h):
        return min(4, size(h, 1))

    def span_of(h, c):
        n = size(h, 1) // parts(h)
        return slice(c * n, (c + 1) * n)

    def piece(h, c, p):
        if h == 0:
            return wgt_s[p, span_of(h, c), 0]
        return wgt_s[span_of(h, c), p, 1]

    def reduce_depth(h, c, sign):
        n = size(h, 2)
        return n // 2 if (c % 2 == 0) == (sign > 0) else n // 2 - 1

    def reduce_round(j):
        for c in range(4):
            for h in range(2):
                if c >= parts(h):
                    continue
                n = size(h, 2)
                part = pl.ds(0, size(h, 1) // parts(h))
                for i, sign in enumerate((1, -1)):
                    depth = reduce_depth(h, c, sign)
                    k = j - (n // 2 - depth)
                    if k < 1 or k > depth:
                        continue
                    dest = lax.rem(place(h, 2) + sign * (depth - k + 1) + n, n)
                    value = piece(h, c, dest)
                    if k > 1:
                        hops[h, c, sign, k - 1].wait_recv()
                        value = value + rs_r[h, c, i, k - 2, part].astype(F32)
                    rs_s[h, c, i, k - 1, part] = value.astype(BF16)
                    hops[h, c, sign, k] = send(
                        rs_s.at[h, c, i, k - 1, part],
                        rs_r.at[h, c, i, k - 1, part],
                        r1_ss.at[h, c, i, k - 1],
                        r1_rs.at[h, c, i, k - 1],
                        along(h, 2, sign),
                    )

    def reduce_finish():
        for c in range(4):
            for h in range(2):
                if c >= parts(h):
                    continue
                value = piece(h, c, place(h, 2))
                part = pl.ds(0, size(h, 1) // parts(h))
                for i, sign in enumerate((1, -1)):
                    depth = reduce_depth(h, c, sign)
                    if depth:
                        hops[h, c, sign, depth].wait_recv()
                        value = value + rs_r[h, c, i, depth - 1, part].astype(F32)
                if h == 0:
                    wgt_s[place(h, 2), span_of(h, c), 0] = value
                else:
                    wgt_s[span_of(h, c), place(h, 2), 1] = value
                q_s[h, span_of(h, c)] = value.astype(BF16)
        todo = [(near(d, size(h, 1)), d, h) for h in range(2) for d in range(1, size(h, 1))]
        for _, d, h in sorted(todo):
            to = lax.rem(place(h, 1) + d, size(h, 1))
            last[h, d] = send(
                q_s.at[h, to], q_r.at[h, d], r2_ss.at[h, d], r2_rs.at[h, d], along(h, 1, d)
            )

    def reduce_end():
        for h in range(2):
            value = wgt_s[z, y, h]
            for d in range(1, size(h, 1)):
                last[h, d].wait_recv()
                value = value + q_r[h, d].astype(F32)
            wg_ref[h] = value

    for r in range(5, rounds - 1):
        gather_round(r)
    reduce_round(1)
    gather_round(rounds - 1)
    reduce_round(2)

    def product_step(i, carry):
        columns = pl.ds(pl.multiple_of(i * block_cols, 128), block_cols)
        part = jnp.dot(
            og_s[:, columns], wt_s[i].reshape(block_cols, width), preferred_element_type=F32
        )
        ag_s[...] = ag_s[...] + part
        return carry

    ag_s[...] = jnp.zeros_like(ag_s)
    lax.fori_loop(0, nz, product_step, 0)

    def pre_step(i, carry):
        gain_sum, bias_sum = carry
        here = pl.ds(pl.multiple_of(i * chunk, 8), chunk)
        normed = conv_s[here, :]
        pre = normed * gain_ref[...] + bias_ref[...]
        gate = jax.nn.sigmoid(pre)
        pre_grad = ag_s[here, :] * gate * (1.0 + pre * (1.0 - gate))
        gain_sum = gain_sum + jnp.sum((pre_grad * normed).reshape(chunk // 8, 8, width), axis=0)
        bias_sum = bias_sum + jnp.sum(pre_grad.reshape(chunk // 8, 8, width), axis=0)
        normed_grad = pre_grad * gain_ref[...]
        ag_s[here, :] = normed_grad
        s1_s[here, :] = fold(normed_grad)
        s2_s[here, :] = fold(normed_grad * normed)
        return gain_sum, bias_sum

    none = jnp.zeros((8, width), F32)
    gain_sum, bias_sum = lax.fori_loop(0, steps, pre_step, (none, none))
    gain_row = jnp.sum(gain_sum, axis=0, keepdims=True)
    bias_row = jnp.sum(bias_sum, axis=0, keepdims=True)
    sums = row_sums(1)
    reduce_round(3)
    total = gathered_sums(1, sums)
    b1_s[...] = down_rows(total[0:1])
    b2_s[...] = down_rows(total[1:2])

    def conv_grad_step(i, carry):
        base = pl.multiple_of(i * chunk, 8)
        here = pl.ds(base, chunk)
        value = wide(ib_s[here, :]) * (
            ag_s[here, :] - wide(b1_s[here, :]) - conv_s[here, :] * wide(b2_s[here, :])
        )
        cgpad[pl.ds(pl.multiple_of(base + EDGE, 8), chunk), :] = value
        return carry

    lax.fori_loop(0, steps, conv_grad_step, 0)
    back = [
        send(cgpad.at[pl.ds(rows, EDGE)], cg_recv.at[0], halo_ss.at[2], halo_rs.at[2], right_dev),
        send(cgpad.at[pl.ds(EDGE, EDGE)], cg_recv.at[1], halo_ss.at[3], halo_rs.at[3], left_dev),
    ]

    tacc[...] = jnp.zeros_like(tacc)

    def tap_step(i, carry):
        base = i * chunk
        value = cgpad[pl.ds(base + EDGE, chunk), :]
        for k in range(span):
            term = value * mpad[pl.ds(base + k + 1, chunk), :]
            tacc[k] = tacc[k] + jnp.sum(term.reshape(chunk // 8, 8, width), axis=0)
        return carry

    for i in range(steps):
        tap_step(i, 0)
    own_small = jnp.concatenate(
        [jnp.sum(tacc[...], axis=1), gain_row, bias_row, jnp.zeros((small_ref.shape[0] - span - 2, width), F32)],
        axis=0,
    )
    small_ref[...] = own_small

    def small_send(phase):
        copies = {}
        for h in range(2):
            ar_s[phase - 1, h] = small_ref[:, h * lanes : (h + 1) * lanes].astype(BF16)
        for h in range(2):
            n = size(h, phase)
            for d in sorted(range(1, n), key=lambda d: near(d, n)):
                copies[h, d] = send(
                    ar_s.at[phase - 1, h],
                    ar_r.at[phase - 1, h, d],
                    ar_ss.at[phase - 1, h, d],
                    ar_rs.at[phase - 1, h, d],
                    along(h, phase, d),
                )
        return copies

    def small_add(phase, copies):
        for h in range(2):
            value = ar_s[phase - 1, h].astype(F32)
            for d in range(1, size(h, phase)):
                copies[h, d].wait_recv()
                value = value + ar_r[phase - 1, h, d].astype(F32)
            small_ref[:, h * lanes : (h + 1) * lanes] = value

    small_1 = small_send(1)
    reduce_round(4)

    back[0].wait_recv()
    back[1].wait_recv()
    cgpad[:EDGE] = jnp.where(s == 0, 0.0, cg_recv[0])
    cgpad[EDGE + rows :] = jnp.where(s == count - 1, 0.0, cg_recv[1])

    def mixed_step(i, carry):
        base = i * chunk
        total = jnp.zeros((chunk, width), F32)
        for k in range(span):
            total = total + taps_ref[k : k + 1, :] * cgpad[pl.ds(base + span - k, chunk), :]
        ag_s[pl.ds(base, chunk), :] = total
        return carry

    for i in range(steps):
        mixed_step(i, 0)
    small_add(1, small_1)
    small_2 = small_send(2)
    reduce_finish()
    scaled = ag_s[...] * sig_s[...]
    vg_ref[...] = scaled.astype(BF16)
    gg_ref[...] = (scaled * vf_s[...] * (1.0 - sig_s[...])).astype(BF16)
    reduce_end()
    small_add(2, small_2)
    for copy in pending:
        copy.wait_send()


def finish(span, vg_ref, gg_ref, small_ref, wg_ref, vg_out, gg_out, tap_out, gain_out, bias_out, wg_out):
    vg_out[...] = vg_ref[...]
    gg_out[...] = gg_ref[...]
    wg_out[...] = wg_ref[...]
    tap_out[...] = small_ref[:span]
    gain_out[...] = small_ref[span : span + 1]
    bias_out[...] = small_ref[span + 1 : span + 2]


def on_device(sizes, value_in, gate_in, taps, norm_gain, norm_bias, proj_weight, out_grad):
    nz, ny, nt = sizes
    rows, width = value_in.shape
    span = taps.shape[0]
    n_col = proj_weight.shape[1]
    quarter = n_col // 2
    columns = out_grad.shape[1]
    lanes = width // 2
    chunk = next(c for c in (72, 24, 8) if rows % c == 0)
    padded_rows = (rows + 127) // 128 * 128
    small_rows = (span + 2 + 15) // 16 * 16
    n_max = max(nz, ny)
    n_half = n_max // 2
    dma = pltpu.SemaphoreType.DMA
    vmem = pl.BlockSpec(memory_space=pltpu.VMEM)
    hbm = pl.BlockSpec(memory_space=pltpu.HBM)
    cfg = (nz, ny, nt, rows, width, span, chunk)
    vg, gg, small, wg = pl.pallas_call(
        functools.partial(kernel, cfg),
        out_shape=(
            jax.ShapeDtypeStruct((rows, width), BF16),
            jax.ShapeDtypeStruct((rows, width), BF16),
            jax.ShapeDtypeStruct((small_rows, width), F32),
            jax.ShapeDtypeStruct((2, quarter, width), F32),
        ),
        in_specs=[hbm] * 7,
        out_specs=(vmem, vmem, vmem, vmem),
        scratch_shapes=[
            pltpu.VMEM((rows, width), BF16),
            pltpu.VMEM((rows, width), BF16),
            pltpu.VMEM((rows, columns), BF16),
            pltpu.VMEM((span, width), F32),
            pltpu.VMEM((1, width), F32),
            pltpu.VMEM((1, width), F32),
            pltpu.VMEM((rows, width), F32),
            pltpu.VMEM((rows, width), F32),
            pltpu.VMEM((rows + 2 * EDGE, width), F32),
            pltpu.VMEM((rows, width), F32),
            pltpu.VMEM((padded_rows, lanes), F32),
            pltpu.VMEM((padded_rows, lanes), F32),
            pltpu.VMEM((padded_rows, lanes), F32),
            pltpu.VMEM((padded_rows, lanes), F32),
            pltpu.VMEM((padded_rows, lanes), F32),
            pltpu.VMEM((rows, width), F32),
            pltpu.VMEM((rows, width), BF16),
            pltpu.VMEM((rows, width), F32),
            pltpu.VMEM((rows + 2 * EDGE, width), F32),
            pltpu.VMEM((span, 8, width), F32),
            pltpu.VMEM((2, EDGE, width), BF16),
            pltpu.VMEM((2, EDGE, width), BF16),
            pltpu.VMEM((2, EDGE, width), F32),
            pltpu.VMEM((2, 2, padded_rows), F32),
            pltpu.VMEM((2, nt, 2, padded_rows), F32),
            pltpu.VMEM((nz, ny, 2, quarter, width), BF16),
            pltpu.VMEM((nz, ny, 2, quarter, width), F32),
            pltpu.VMEM((2, 4, 2, n_half, max(1, n_max // 4), quarter, width), BF16),
            pltpu.VMEM((2, 4, 2, n_half, max(1, n_max // 4), quarter, width), BF16),
            pltpu.VMEM((2, n_max, quarter, width), BF16),
            pltpu.VMEM((2, n_max, quarter, width), BF16),
            pltpu.VMEM((2, 2, small_rows, lanes), BF16),
            pltpu.VMEM((2, 2, n_max, small_rows, lanes), BF16),
            dma((7,)),
            dma((4,)),
            dma((4,)),
            dma((2, nt)),
            dma((2, nt)),
            dma((2, n_max)),
            dma((2, n_max)),
            dma((2, n_max, 2, n_half)),
            dma((2, n_max, 2, n_half)),
            dma((2, 4, 2, n_half)),
            dma((2, 4, 2, n_half)),
            dma((2, n_max)),
            dma((2, n_max)),
            dma((2, 2, n_max)),
            dma((2, 2, n_max)),
        ],
        compiler_params=pltpu.CompilerParams(
            collective_id=0, has_side_effects=True, vmem_limit_bytes=60 * 1024 * 1024
        ),
        name="step",
    )(
        value_in,
        gate_in,
        taps,
        norm_gain[None, :],
        norm_bias[None, :],
        proj_weight.T.reshape(2, quarter, width),
        out_grad,
    )
    vg, gg, tap, gain, bias, wg = pl.pallas_call(
        functools.partial(finish, span),
        out_shape=(
            jax.ShapeDtypeStruct((rows, width), BF16),
            jax.ShapeDtypeStruct((rows, width), BF16),
            jax.ShapeDtypeStruct((span, width), F32),
            jax.ShapeDtypeStruct((1, width), F32),
            jax.ShapeDtypeStruct((1, width), F32),
            jax.ShapeDtypeStruct((2, quarter, width), F32),
        ),
        in_specs=[vmem] * 4,
        out_specs=(vmem,) * 6,
        compiler_params=pltpu.CompilerParams(vmem_limit_bytes=60 * 1024 * 1024),
        name="finish",
    )(vg, gg, small, wg)
    return (vg, gg, tap, gain[0], bias[0], jnp.transpose(wg.reshape(n_col, width)))


def solution(mesh):
    tp = mesh.shape["tp"]
    ny = 8 if mesh.shape["sp"] % 8 == 0 else 2
    nz = mesh.shape["sp"] // ny
    finer = Mesh(mesh.devices.reshape(nz, ny, tp), (*SP, "tp"))
    in_specs = (P(SP, "tp"), P(SP, "tp"), P(None, "tp"), P("tp"), P("tp"), P("tp", SP), P(SP, None))
    out_specs = (P(SP, "tp"), P(SP, "tp"), P(None, "tp"), P("tp"), P("tp"), P("tp", SP))
    return jax.shard_map(
        functools.partial(on_device, (nz, ny, tp)),
        mesh=finer,
        in_specs=in_specs,
        out_specs=out_specs,
        check_vma=False,
    )
```

```python
import functools

import jax
import jax.numpy as jnp
from jax import lax
from jax.experimental import pallas as pl
from jax.experimental.pallas import tpu as pltpu
from jax.sharding import Mesh
from jax.sharding import PartitionSpec as P

SP = ("sp_0", "sp_1")
MESH = pl.DeviceIdType.MESH
EPS = 1e-06
F32 = jnp.float32
BF16 = jnp.bfloat16
EDGE = 16


def kernel(
    cfg,
    v_hbm,
    g_hbm,
    taps_hbm,
    gain_hbm,
    bias_hbm,
    w_hbm,
    og_hbm,
    vg_hbm,
    gg_hbm,
    small_ref,
    wg_ref,
    v_s,
    g_s,
    og_s,
    taps_ref,
    gain_ref,
    bias_ref,
    vf_s,
    sig_s,
    mpad,
    conv_s,
    s1_s,
    s2_s,
    b1_s,
    b2_s,
    ib_s,
    act_f,
    act_s,
    ag_s,
    cgpad,
    tacc,
    halo_send,
    halo_recv,
    cg_recv,
    st_send,
    st_recv,
    wt_s,
    wgt_s,
    rs_s,
    rs_r,
    q_s,
    q_r,
    ar_s,
    ar_r,
    local_sem,
    halo_ss,
    halo_rs,
    st_ss,
    st_rs,
    a1_ss,
    a1_rs,
    a2_ss,
    a2_rs,
    r1_ss,
    r1_rs,
    r2_ss,
    r2_rs,
    ar_ss,
    ar_rs,
):
    nz, ny, nt, rows, width, span, chunk = cfg
    z, y, t = lax.axis_index("sp_0"), lax.axis_index("sp_1"), lax.axis_index("tp")
    count = nz * ny
    s = z * ny + y
    lanes = width // 2
    channels = width * nt
    steps = rows // chunk
    padded_rows = s1_s.shape[0]
    quarter = w_hbm.shape[1]
    n_col = 2 * quarter

    def at(zz, yy, tt):
        return (zz, yy, tt)

    def along(h, phase, shift):
        on_y = (h == 0) == (phase == 1)
        if on_y:
            return at(z, lax.rem(y + shift + ny, ny), t)
        return at(lax.rem(z + shift + nz, nz), y, t)

    def size(h, phase):
        return ny if (h == 0) == (phase == 1) else nz

    def place(h, phase):
        return y if (h == 0) == (phase == 1) else z

    def cell(h, a, b):
        return (b, a) if h == 0 else (a, b)

    pending = []

    def send(src, dst, ssem, rsem, dev):
        copy = pltpu.make_async_remote_copy(
            src_ref=src, dst_ref=dst, send_sem=ssem, recv_sem=rsem, device_id=dev, device_id_type=MESH
        )
        copy.start()
        pending.append(copy)
        return copy

    load_v = pltpu.make_async_copy(v_hbm, v_s, local_sem.at[0])
    load_g = pltpu.make_async_copy(g_hbm, g_s, local_sem.at[1])
    load_og = pltpu.make_async_copy(og_hbm, og_s, local_sem.at[2])
    load_w = pltpu.make_async_copy(w_hbm, wt_s.at[z, y], local_sem.at[3])
    load_taps = pltpu.make_async_copy(taps_hbm, taps_ref, local_sem.at[4])
    load_gain = pltpu.make_async_copy(gain_hbm, gain_ref, local_sem.at[5])
    load_bias = pltpu.make_async_copy(bias_hbm, bias_ref, local_sem.at[6])
    for load in (load_g, load_v, load_w, load_taps, load_gain, load_bias, load_og):
        load.start()

    right = lax.rem(s + 1, count)
    left = lax.rem(s + count - 1, count)
    right_dev = at(right // ny, lax.rem(right, ny), t)
    left_dev = at(left // ny, lax.rem(left, ny), t)
    barrier = pltpu.get_barrier_semaphore()
    peers = [right_dev, left_dev]
    peers += [at(z, lax.rem(y + d, ny), t) for d in range(1, ny)]
    peers += [at(lax.rem(z + d, nz), y, t) for d in range(1, nz)]
    peers += [at(z, y, lax.rem(t + d, nt)) for d in range(1, nt)]
    for dev in peers:
        pl.semaphore_signal(barrier, inc=1, device_id=dev, device_id_type=MESH)

    load_g.wait()
    load_v.wait()
    sig = jax.nn.sigmoid(g_s[...].astype(F32))
    sig_s[...] = sig
    vf = v_s[...].astype(F32)
    vf_s[...] = vf
    mixed = (vf * sig).astype(BF16)
    halo_send[0] = mixed[rows - EDGE :]
    halo_send[1] = mixed[:EDGE]
    mpad[EDGE : EDGE + rows] = mixed.astype(F32)

    for load in (load_w, load_taps, load_gain, load_bias):
        load.wait()
    pl.semaphore_wait(barrier, len(peers))

    halo = [
        send(halo_send.at[0], halo_recv.at[0], halo_ss.at[0], halo_rs.at[0], right_dev),
        send(halo_send.at[1], halo_recv.at[1], halo_ss.at[1], halo_rs.at[1], left_dev),
    ]

    first, ring = {}, {}

    def near(d, n):
        return min(d, n - d)

    def ring_depth(h, d, sign):
        n = size(h, 2)
        even = d % 2 == 0
        return n // 2 if even == (sign > 0) else n // 2 - 1

    def forward(h, d, sign, k):
        a = lax.rem(place(h, 1) - d + size(h, 1), size(h, 1))
        n = size(h, 2)
        b = lax.rem(place(h, 2) - sign * (k - 1) + n, n)
        block = wt_s.at[(*cell(h, a, b), h)]
        i = 0 if sign > 0 else 1
        ring[h, d, sign, k] = send(
            block, block, a2_ss.at[h, d, i, k - 1], a2_rs.at[h, d, i, k - 1], along(h, 2, sign)
        )

    def gather_start():
        for h in range(2):
            for sign in (1, -1):
                if ring_depth(h, 0, sign) >= 1:
                    forward(h, 0, sign, 1)
        todo = [(near(d, size(h, 1)), d, h) for h in range(2) for d in range(1, size(h, 1))]
        for _, d, h in sorted(todo):
            block = wt_s.at[(*cell(h, place(h, 1), place(h, 2)), h)]
            first[h, d] = send(block, block, a1_ss.at[h, d], a1_rs.at[h, d], along(h, 1, d))

    def gather_round(r, low=0, high=99):
        todo = []
        for h in range(2):
            n = size(h, 1)
            for d in range(n):
                k = r - min(near(d, n), 1) + 1
                if (d == 0 and k == 1) or k < 1 or k > size(h, 2) // 2 + 1 or not low <= near(d, n) <= high:
                    continue
                todo.append((near(d, n), d, h, k))
        for _, d, h, k in sorted(todo):
            if k == 1:
                first[h, d].wait_recv()
            for sign in (1, -1):
                depth = ring_depth(h, d, sign)
                if 1 <= k - 1 <= depth:
                    ring[h, d, sign, k - 1].wait_recv()
                if k <= depth:
                    forward(h, d, sign, k)

    rounds = max(size(h, 2) // 2 + 2 for h in range(2))
    gather_start()
    gather_round(1, 0, 2)

    halo[0].wait_recv()
    halo[1].wait_recv()
    gather_round(1, 3)
    mpad[:EDGE] = jnp.where(s == 0, 0.0, halo_recv[0].astype(F32))
    mpad[EDGE + rows :] = jnp.where(s == count - 1, 0.0, halo_recv[1].astype(F32))

    def fold(x):
        return x[:, :lanes] + x[:, lanes:]

    def wide(x):
        return jnp.concatenate([x, x], axis=1)

    def conv_step(i, carry):
        base = i * chunk
        total = jnp.zeros((chunk, width), F32)
        for k in range(span):
            total = total + taps_ref[k : k + 1, :] * mpad[pl.ds(base + k + 1, chunk), :]
        conv_s[pl.ds(base, chunk), :] = total
        s1_s[pl.ds(base, chunk), :] = fold(total)
        s2_s[pl.ds(base, chunk), :] = fold(total * total)
        return carry

    for i in range(steps):
        conv_step(i, 0)

    def row_sums(which):
        a = jnp.sum(jnp.transpose(s1_s[...]), axis=0, keepdims=True)
        b = jnp.sum(jnp.transpose(s2_s[...]), axis=0, keepdims=True)
        both = jnp.concatenate([a, b], axis=0)
        st_send[which] = both
        copies = []
        for d in range(1, nt):
            copies.append(
                send(
                    st_send.at[which],
                    st_recv.at[which, d],
                    st_ss.at[which, d],
                    st_rs.at[which, d],
                    at(z, y, lax.rem(t + d, nt)),
                )
            )
        return copies

    def gathered_sums(which, copies):
        total = st_send[which]
        for d in range(1, nt):
            copies[d - 1].wait_recv()
            total = total + st_recv[which, d]
        return total / channels

    def down_rows(row):
        return jnp.transpose(jnp.broadcast_to(row, (lanes, padded_rows)))

    sums = row_sums(0)
    gather_round(2)
    gather_round(3)
    total = gathered_sums(0, sums)
    mean = total[0:1]
    inv = lax.rsqrt(total[1:2] - mean * mean + EPS)
    b1_s[...] = down_rows(mean)
    ib_s[...] = down_rows(inv)

    def act_step(i, carry):
        here = pl.ds(pl.multiple_of(i * chunk, 8), chunk)
        normed = (conv_s[here, :] - wide(b1_s[here, :])) * wide(ib_s[here, :])
        conv_s[here, :] = normed
        pre = normed * gain_ref[...] + bias_ref[...]
        act_f[here, :] = pre * jax.nn.sigmoid(pre)
        return carry

    lax.fori_loop(0, steps, act_step, 0)
    act_s[...] = act_f[...].astype(BF16)
    load_og.wait()

    block_cols = ny * n_col

    def grad_step(i, carry):
        columns = pl.ds(pl.multiple_of(i * block_cols, 128), block_cols)
        part = lax.dot_general(
            og_s[:, columns], act_s[...], (((0,), (0,)), ((), ())), preferred_element_type=F32
        )
        wgt_s[i] = part.reshape(ny, 2, quarter, width)
        return carry

    lax.fori_loop(0, nz // 2, grad_step, 0)
    gather_round(4)
    lax.fori_loop(nz // 2, nz, grad_step, 0)

    hops, last = {}, {}

    def parts(h):
        return min(4, size(h, 1))

    def span_of(h, c):
        n = size(h, 1) // parts(h)
        return slice(c * n, (c + 1) * n)

    def piece(h, c, p):
        if h == 0:
            return wgt_s[p, span_of(h, c), 0]
        return wgt_s[span_of(h, c), p, 1]

    def reduce_depth(h, c, sign):
        n = size(h, 2)
        return n // 2 if (c % 2 == 0) == (sign > 0) else n // 2 - 1

    def reduce_round(j):
        for c in range(4):
            for h in range(2):
                if c >= parts(h):
                    continue
                n = size(h, 2)
                part = pl.ds(0, size(h, 1) // parts(h))
                for i, sign in enumerate((1, -1)):
                    depth = reduce_depth(h, c, sign)
                    k = j - (n // 2 - depth)
                    if k < 1 or k > depth:
                        continue
                    dest = lax.rem(place(h, 2) + sign * (depth - k + 1) + n, n)
                    value = piece(h, c, dest)
                    if k > 1:
                        hops[h, c, sign, k - 1].wait_recv()
                        value = value + rs_r[h, c, i, k - 2, part].astype(F32)
                    rs_s[h, c, i, k - 1, part] = value.astype(BF16)
                    hops[h, c, sign, k] = send(
                        rs_s.at[h, c, i, k - 1, part],
                        rs_r.at[h, c, i, k - 1, part],
                        r1_ss.at[h, c, i, k - 1],
                        r1_rs.at[h, c, i, k - 1],
                        along(h, 2, sign),
                    )

    def reduce_finish():
        for c in range(4):
            for h in range(2):
                if c >= parts(h):
                    continue
                value = piece(h, c, place(h, 2))
                part = pl.ds(0, size(h, 1) // parts(h))
                for i, sign in enumerate((1, -1)):
                    depth = reduce_depth(h, c, sign)
                    if depth:
                        hops[h, c, sign, depth].wait_recv()
                        value = value + rs_r[h, c, i, depth - 1, part].astype(F32)
                if h == 0:
                    wgt_s[place(h, 2), span_of(h, c), 0] = value
                else:
                    wgt_s[span_of(h, c), place(h, 2), 1] = value
                q_s[h, span_of(h, c)] = value.astype(BF16)
        todo = [(-near(d, size(h, 1)), d, h) for h in range(2) for d in range(1, size(h, 1))]
        for _, d, h in sorted(todo):
            to = lax.rem(place(h, 1) + d, size(h, 1))
            last[h, d] = send(
                q_s.at[h, to], q_r.at[h, d], r2_ss.at[h, d], r2_rs.at[h, d], along(h, 1, d)
            )

    def reduce_end():
        for h in range(2):
            value = wgt_s[z, y, h]
            for d in range(1, size(h, 1)):
                last[h, d].wait_recv()
                value = value + q_r[h, d].astype(F32)
            wg_ref[h] = value

    for r in range(5, rounds - 1):
        gather_round(r)
    reduce_round(1)
    gather_round(rounds - 1)

    def product_step(i, carry):
        columns = pl.ds(pl.multiple_of(i * block_cols, 128), block_cols)
        part = jnp.dot(
            og_s[:, columns], wt_s[i].reshape(block_cols, width), preferred_element_type=F32
        )
        ag_s[...] = ag_s[...] + part
        return carry

    ag_s[...] = jnp.zeros_like(ag_s)
    lax.fori_loop(0, nz, product_step, 0)
    reduce_round(2)

    def pre_step(i, carry):
        gain_sum, bias_sum = carry
        here = pl.ds(pl.multiple_of(i * chunk, 8), chunk)
        normed = conv_s[here, :]
        pre = normed * gain_ref[...] + bias_ref[...]
        gate = jax.nn.sigmoid(pre)
        pre_grad = ag_s[here, :] * gate * (1.0 + pre * (1.0 - gate))
        gain_sum = gain_sum + jnp.sum((pre_grad * normed).reshape(chunk // 8, 8, width), axis=0)
        bias_sum = bias_sum + jnp.sum(pre_grad.reshape(chunk // 8, 8, width), axis=0)
        normed_grad = pre_grad * gain_ref[...]
        ag_s[here, :] = normed_grad
        s1_s[here, :] = fold(normed_grad)
        s2_s[here, :] = fold(normed_grad * normed)
        return gain_sum, bias_sum

    none = jnp.zeros((8, width), F32)
    gain_sum, bias_sum = lax.fori_loop(0, steps, pre_step, (none, none))
    gain_row = jnp.sum(gain_sum, axis=0, keepdims=True)
    bias_row = jnp.sum(bias_sum, axis=0, keepdims=True)
    sums = row_sums(1)
    reduce_round(3)
    total = gathered_sums(1, sums)
    b1_s[...] = down_rows(total[0:1])
    b2_s[...] = down_rows(total[1:2])

    def conv_grad_step(i, carry):
        base = pl.multiple_of(i * chunk, 8)
        here = pl.ds(base, chunk)
        value = wide(ib_s[here, :]) * (
            ag_s[here, :] - wide(b1_s[here, :]) - conv_s[here, :] * wide(b2_s[here, :])
        )
        cgpad[pl.ds(pl.multiple_of(base + EDGE, 8), chunk), :] = value
        return carry

    lax.fori_loop(0, steps, conv_grad_step, 0)
    back = [
        send(cgpad.at[pl.ds(rows, EDGE)], cg_recv.at[0], halo_ss.at[2], halo_rs.at[2], right_dev),
        send(cgpad.at[pl.ds(EDGE, EDGE)], cg_recv.at[1], halo_ss.at[3], halo_rs.at[3], left_dev),
    ]

    tacc[...] = jnp.zeros_like(tacc)

    def tap_step(i, carry):
        base = i * chunk
        value = cgpad[pl.ds(base + EDGE, chunk), :]
        for k in range(span):
            term = value * mpad[pl.ds(base + k + 1, chunk), :]
            tacc[k] = tacc[k] + jnp.sum(term.reshape(chunk // 8, 8, width), axis=0)
        return carry

    for i in range(steps):
        tap_step(i, 0)
    own_small = jnp.concatenate(
        [jnp.sum(tacc[...], axis=1), gain_row, bias_row, jnp.zeros((small_ref.shape[0] - span - 2, width), F32)],
        axis=0,
    )
    small_ref[...] = own_small

    def small_send(phase):
        copies = {}
        for h in range(2):
            ar_s[phase - 1, h] = small_ref[:, h * lanes : (h + 1) * lanes].astype(BF16)
        todo = [(-near(d, size(h, phase)), d, h) for h in range(2) for d in range(1, size(h, phase))]
        for _, d, h in sorted(todo):
            copies[h, d] = send(
                ar_s.at[phase - 1, h],
                ar_r.at[phase - 1, h, d],
                ar_ss.at[phase - 1, h, d],
                ar_rs.at[phase - 1, h, d],
                along(h, phase, d),
            )
        return copies

    def small_add(phase, copies):
        for h in range(2):
            value = ar_s[phase - 1, h].astype(F32)
            for d in range(1, size(h, phase)):
                copies[h, d].wait_recv()
                value = value + ar_r[phase - 1, h, d].astype(F32)
            small_ref[:, h * lanes : (h + 1) * lanes] = value

    small_1 = small_send(1)
    reduce_round(4)

    back[0].wait_recv()
    back[1].wait_recv()
    cgpad[:EDGE] = jnp.where(s == 0, 0.0, cg_recv[0])
    cgpad[EDGE + rows :] = jnp.where(s == count - 1, 0.0, cg_recv[1])

    def mixed_step(i, carry):
        base = i * chunk
        total = jnp.zeros((chunk, width), F32)
        for k in range(span):
            total = total + taps_ref[k : k + 1, :] * cgpad[pl.ds(base + span - k, chunk), :]
        ag_s[pl.ds(base, chunk), :] = total
        return carry

    for i in range(steps):
        mixed_step(i, 0)
    reduce_finish()
    small_add(1, small_1)
    small_2 = small_send(2)
    scaled = ag_s[...] * sig_s[...]
    v_s[...] = scaled.astype(BF16)
    g_s[...] = (scaled * vf_s[...] * (1.0 - sig_s[...])).astype(BF16)
    store_v = pltpu.make_async_copy(v_s, vg_hbm, local_sem.at[0])
    store_g = pltpu.make_async_copy(g_s, gg_hbm, local_sem.at[1])
    store_v.start()
    store_g.start()
    reduce_end()
    small_add(2, small_2)
    store_v.wait()
    store_g.wait()
    for copy in pending:
        copy.wait_send()


def finish(span, vg_ref, gg_ref, small_ref, wg_ref, vg_out, gg_out, tap_out, gain_out, bias_out, wg_out):
    vg_out[...] = vg_ref[...]
    gg_out[...] = gg_ref[...]
    wg_out[...] = wg_ref[...]
    tap_out[...] = small_ref[:span]
    gain_out[...] = small_ref[span : span + 1]
    bias_out[...] = small_ref[span + 1 : span + 2]


def on_device(sizes, value_in, gate_in, taps, norm_gain, norm_bias, proj_weight, out_grad):
    nz, ny, nt = sizes
    rows, width = value_in.shape
    span = taps.shape[0]
    n_col = proj_weight.shape[1]
    quarter = n_col // 2
    columns = out_grad.shape[1]
    lanes = width // 2
    chunk = next(c for c in (72, 24, 8) if rows % c == 0)
    padded_rows = (rows + 127) // 128 * 128
    small_rows = (span + 2 + 7) // 8 * 8
    n_max = max(nz, ny)
    n_half = n_max // 2
    dma = pltpu.SemaphoreType.DMA
    vmem = pl.BlockSpec(memory_space=pltpu.VMEM)
    hbm = pl.BlockSpec(memory_space=pltpu.HBM)
    cfg = (nz, ny, nt, rows, width, span, chunk)
    vg, gg, small, wg = pl.pallas_call(
        functools.partial(kernel, cfg),
        out_shape=(
            jax.ShapeDtypeStruct((rows, width), BF16),
            jax.ShapeDtypeStruct((rows, width), BF16),
            jax.ShapeDtypeStruct((small_rows, width), F32),
            jax.ShapeDtypeStruct((2, quarter, width), F32),
        ),
        in_specs=[hbm] * 7,
        out_specs=(hbm, hbm, vmem, vmem),
        scratch_shapes=[
            pltpu.VMEM((rows, width), BF16),
            pltpu.VMEM((rows, width), BF16),
            pltpu.VMEM((rows, columns), BF16),
            pltpu.VMEM((span, width), F32),
            pltpu.VMEM((1, width), F32),
            pltpu.VMEM((1, width), F32),
            pltpu.VMEM((rows, width), F32),
            pltpu.VMEM((rows, width), F32),
            pltpu.VMEM((rows + 2 * EDGE, width), F32),
            pltpu.VMEM((rows, width), F32),
            pltpu.VMEM((padded_rows, lanes), F32),
            pltpu.VMEM((padded_rows, lanes), F32),
            pltpu.VMEM((padded_rows, lanes), F32),
            pltpu.VMEM((padded_rows, lanes), F32),
            pltpu.VMEM((padded_rows, lanes), F32),
            pltpu.VMEM((rows, width), F32),
            pltpu.VMEM((rows, width), BF16),
            pltpu.VMEM((rows, width), F32),
            pltpu.VMEM((rows + 2 * EDGE, width), F32),
            pltpu.VMEM((span, 8, width), F32),
            pltpu.VMEM((2, EDGE, width), BF16),
            pltpu.VMEM((2, EDGE, width), BF16),
            pltpu.VMEM((2, EDGE, width), F32),
            pltpu.VMEM((2, 2, padded_rows), F32),
            pltpu.VMEM((2, nt, 2, padded_rows), F32),
            pltpu.VMEM((nz, ny, 2, quarter, width), BF16),
            pltpu.VMEM((nz, ny, 2, quarter, width), F32),
            pltpu.VMEM((2, 4, 2, n_half, max(1, n_max // 4), quarter, width), BF16),
            pltpu.VMEM((2, 4, 2, n_half, max(1, n_max // 4), quarter, width), BF16),
            pltpu.VMEM((2, n_max, quarter, width), BF16),
            pltpu.VMEM((2, n_max, quarter, width), BF16),
            pltpu.VMEM((2, 2, small_rows, lanes), BF16),
            pltpu.VMEM((2, 2, n_max, small_rows, lanes), BF16),
            dma((7,)),
            dma((4,)),
            dma((4,)),
            dma((2, nt)),
            dma((2, nt)),
            dma((2, n_max)),
            dma((2, n_max)),
            dma((2, n_max, 2, n_half)),
            dma((2, n_max, 2, n_half)),
            dma((2, 4, 2, n_half)),
            dma((2, 4, 2, n_half)),
            dma((2, n_max)),
            dma((2, n_max)),
            dma((2, 2, n_max)),
            dma((2, 2, n_max)),
        ],
        compiler_params=pltpu.CompilerParams(
            collective_id=0, has_side_effects=True, vmem_limit_bytes=60 * 1024 * 1024
        ),
        name="step",
    )(
        value_in,
        gate_in,
        taps,
        norm_gain[None, :],
        norm_bias[None, :],
        proj_weight.T.reshape(2, quarter, width),
        out_grad,
    )
    vg, gg, tap, gain, bias, wg = pl.pallas_call(
        functools.partial(finish, span),
        out_shape=(
            jax.ShapeDtypeStruct((rows, width), BF16),
            jax.ShapeDtypeStruct((rows, width), BF16),
            jax.ShapeDtypeStruct((span, width), F32),
            jax.ShapeDtypeStruct((1, width), F32),
            jax.ShapeDtypeStruct((1, width), F32),
            jax.ShapeDtypeStruct((2, quarter, width), F32),
        ),
        in_specs=[vmem] * 4,
        out_specs=(vmem,) * 6,
        compiler_params=pltpu.CompilerParams(vmem_limit_bytes=60 * 1024 * 1024),
        name="finish",
    )(vg, gg, small, wg)
    return (vg, gg, tap, gain[0], bias[0], jnp.transpose(wg.reshape(n_col, width)))


def solution(mesh):
    tp = mesh.shape["tp"]
    ny = 8 if mesh.shape["sp"] % 8 == 0 else 2
    nz = mesh.shape["sp"] // ny
    finer = Mesh(mesh.devices.reshape(nz, ny, tp), (*SP, "tp"))
    in_specs = (P(SP, "tp"), P(SP, "tp"), P(None, "tp"), P("tp"), P("tp"), P("tp", SP), P(SP, None))
    out_specs = (P(SP, "tp"), P(SP, "tp"), P(None, "tp"), P("tp"), P("tp"), P("tp", SP))
    return jax.shard_map(
        functools.partial(on_device, (nz, ny, tp)),
        mesh=finer,
        in_specs=in_specs,
        out_specs=out_specs,
        check_vma=False,
    )
```

```python
import functools

import jax
import jax.numpy as jnp
from jax import lax
from jax.experimental import pallas as pl
from jax.experimental.pallas import tpu as pltpu
from jax.sharding import Mesh
from jax.sharding import PartitionSpec as P

SP = ("sp_0", "sp_1")
MESH = pl.DeviceIdType.MESH
EPS = 1e-06
F32 = jnp.float32
BF16 = jnp.bfloat16
EDGE = 16


def kernel(
    cfg,
    v_hbm,
    g_hbm,
    taps_hbm,
    gain_hbm,
    bias_hbm,
    w_hbm,
    og_hbm,
    vg_hbm,
    gg_hbm,
    small_ref,
    wg_ref,
    v_s,
    g_s,
    og_s,
    taps_ref,
    gain_ref,
    bias_ref,
    vf_s,
    sig_s,
    mpad,
    conv_s,
    s1_s,
    s2_s,
    b1_s,
    b2_s,
    ib_s,
    act_f,
    act_s,
    ag_s,
    cgpad,
    tacc,
    halo_send,
    halo_recv,
    cg_recv,
    st_send,
    st_recv,
    wt_s,
    wgt_s,
    rs_s,
    rs_r,
    q_s,
    q_r,
    ar_s,
    ar_r,
    local_sem,
    send_sem,
    halo_rs,
    st_rs,
    a1_rs,
    a2_rs,
    r2_rs,
    ar_rs,
):
    nz, ny, nt, rows, width, span, chunk = cfg
    z, y, t = lax.axis_index("sp_0"), lax.axis_index("sp_1"), lax.axis_index("tp")
    count = nz * ny
    s = z * ny + y
    lanes = width // 2
    channels = width * nt
    steps = rows // chunk
    padded_rows = s1_s.shape[0]
    quarter = w_hbm.shape[1]
    n_col = 2 * quarter

    def at(zz, yy, tt):
        return (zz, yy, tt)

    def along(h, phase, shift):
        on_y = (h == 0) == (phase == 1)
        if on_y:
            return at(z, lax.rem(y + shift + ny, ny), t)
        return at(lax.rem(z + shift + nz, nz), y, t)

    def size(h, phase):
        return ny if (h == 0) == (phase == 1) else nz

    def place(h, phase):
        return y if (h == 0) == (phase == 1) else z

    def cell(h, a, b):
        return (b, a) if h == 0 else (a, b)

    pending = []
    slots = send_sem.shape[0]

    def send(src, dst, rsem, dev):
        slot = len(pending) % slots
        if len(pending) >= slots:
            pending[-slots].wait_send()
        copy = pltpu.make_async_remote_copy(
            src_ref=src,
            dst_ref=dst,
            send_sem=send_sem.at[slot],
            recv_sem=rsem,
            device_id=dev,
            device_id_type=MESH,
        )
        copy.start()
        pending.append(copy)
        return copy

    load_v = pltpu.make_async_copy(v_hbm, v_s, local_sem.at[0])
    load_g = pltpu.make_async_copy(g_hbm, g_s, local_sem.at[1])
    load_og = pltpu.make_async_copy(og_hbm, og_s, local_sem.at[2])
    load_w = pltpu.make_async_copy(w_hbm, wt_s.at[z, y], local_sem.at[3])
    load_taps = pltpu.make_async_copy(taps_hbm, taps_ref, local_sem.at[4])
    load_gain = pltpu.make_async_copy(gain_hbm, gain_ref, local_sem.at[5])
    load_bias = pltpu.make_async_copy(bias_hbm, bias_ref, local_sem.at[6])
    for load in (load_g, load_v, load_w, load_taps, load_gain, load_bias, load_og):
        load.start()

    right = lax.rem(s + 1, count)
    left = lax.rem(s + count - 1, count)
    right_dev = at(right // ny, lax.rem(right, ny), t)
    left_dev = at(left // ny, lax.rem(left, ny), t)
    barrier = pltpu.get_barrier_semaphore()
    peers = [right_dev, left_dev]
    peers += [at(z, lax.rem(y + d, ny), t) for d in range(1, ny)]
    peers += [at(lax.rem(z + d, nz), y, t) for d in range(1, nz)]
    peers += [at(z, y, lax.rem(t + d, nt)) for d in range(1, nt)]
    for dev in peers:
        pl.semaphore_signal(barrier, inc=1, device_id=dev, device_id_type=MESH)

    load_g.wait()
    load_v.wait()
    sig = jax.nn.sigmoid(g_s[...].astype(F32))
    sig_s[...] = sig
    vf = v_s[...].astype(F32)
    vf_s[...] = vf
    mixed = (vf * sig).astype(BF16)
    halo_send[0] = mixed[rows - EDGE :]
    halo_send[1] = mixed[:EDGE]
    mpad[EDGE : EDGE + rows] = mixed.astype(F32)

    for load in (load_w, load_taps, load_gain, load_bias):
        load.wait()
    pl.semaphore_wait(barrier, len(peers))

    halo = [
        send(halo_send.at[0], halo_recv.at[0], halo_rs.at[0], right_dev),
        send(halo_send.at[1], halo_recv.at[1], halo_rs.at[1], left_dev),
    ]

    first, ring = {}, {}

    def near(d, n):
        return min(d, n - d)

    def ring_depth(h, d, sign):
        n = size(h, 2)
        even = d % 2 == 0
        return n // 2 if even == (sign > 0) else n // 2 - 1

    def forward(h, d, sign, k):
        a = lax.rem(place(h, 1) - d + size(h, 1), size(h, 1))
        n = size(h, 2)
        b = lax.rem(place(h, 2) - sign * (k - 1) + n, n)
        block = wt_s.at[(*cell(h, a, b), h)]
        i = 0 if sign > 0 else 1
        ring[h, d, sign, k] = send(
            block, block, a2_rs.at[h, d, i, k - 1], along(h, 2, sign)
        )

    def gather_start():
        for h in range(2):
            for sign in (1, -1):
                if ring_depth(h, 0, sign) >= 1:
                    forward(h, 0, sign, 1)
        todo = [(near(d, size(h, 1)), d, h) for h in range(2) for d in range(1, size(h, 1))]
        for _, d, h in sorted(todo):
            block = wt_s.at[(*cell(h, place(h, 1), place(h, 2)), h)]
            first[h, d] = send(block, block, a1_rs.at[h, d], along(h, 1, d))

    def gather_round(r, low=0, high=99):
        todo = []
        for h in range(2):
            n = size(h, 1)
            for d in range(n):
                k = r - min(near(d, n), 1) + 1
                if (d == 0 and k == 1) or k < 1 or k > size(h, 2) // 2 + 1 or not low <= near(d, n) <= high:
                    continue
                todo.append((near(d, n), d, h, k))
        for _, d, h, k in sorted(todo):
            if k == 1:
                first[h, d].wait_recv()
            for sign in (1, -1):
                depth = ring_depth(h, d, sign)
                if 1 <= k - 1 <= depth:
                    ring[h, d, sign, k - 1].wait_recv()
                if k <= depth:
                    forward(h, d, sign, k)

    rounds = max(size(h, 2) // 2 + 2 for h in range(2))
    gather_start()
    gather_round(1, 0, 2)

    halo[0].wait_recv()
    halo[1].wait_recv()
    gather_round(1, 3)
    mpad[:EDGE] = jnp.where(s == 0, 0.0, halo_recv[0].astype(F32))
    mpad[EDGE + rows :] = jnp.where(s == count - 1, 0.0, halo_recv[1].astype(F32))

    def fold(x):
        return x[:, :lanes] + x[:, lanes:]

    def wide(x):
        return jnp.concatenate([x, x], axis=1)

    def conv_step(i, carry):
        base = i * chunk
        total = jnp.zeros((chunk, width), F32)
        for k in range(span):
            total = total + taps_ref[k : k + 1, :] * mpad[pl.ds(base + k + 1, chunk), :]
        conv_s[pl.ds(base, chunk), :] = total
        s1_s[pl.ds(base, chunk), :] = fold(total)
        s2_s[pl.ds(base, chunk), :] = fold(total * total)
        return carry

    for i in range(steps):
        conv_step(i, 0)

    def row_sums(which):
        a = jnp.sum(jnp.transpose(s1_s[...]), axis=0, keepdims=True)
        b = jnp.sum(jnp.transpose(s2_s[...]), axis=0, keepdims=True)
        both = jnp.concatenate([a, b], axis=0)
        st_send[which] = both
        copies = []
        for d in range(1, nt):
            copies.append(
                send(
                    st_send.at[which],
                    st_recv.at[which, d],
                    st_rs.at[which, d],
                    at(z, y, lax.rem(t + d, nt)),
                )
            )
        return copies

    def gathered_sums(which, copies):
        total = st_send[which]
        for d in range(1, nt):
            copies[d - 1].wait_recv()
            total = total + st_recv[which, d]
        return total / channels

    def down_rows(row):
        return jnp.transpose(jnp.broadcast_to(row, (lanes, padded_rows)))

    sums = row_sums(0)
    gather_round(2)
    gather_round(3)
    total = gathered_sums(0, sums)
    mean = total[0:1]
    inv = lax.rsqrt(total[1:2] - mean * mean + EPS)
    b1_s[...] = down_rows(mean)
    ib_s[...] = down_rows(inv)

    def act_step(i, carry):
        here = pl.ds(pl.multiple_of(i * chunk, 8), chunk)
        normed = (conv_s[here, :] - wide(b1_s[here, :])) * wide(ib_s[here, :])
        conv_s[here, :] = normed
        pre = normed * gain_ref[...] + bias_ref[...]
        act_f[here, :] = pre * jax.nn.sigmoid(pre)
        return carry

    lax.fori_loop(0, steps, act_step, 0)
    act_s[...] = act_f[...].astype(BF16)
    load_og.wait()

    block_cols = ny * n_col

    def grad_step(i, carry):
        columns = pl.ds(pl.multiple_of(i * block_cols, 128), block_cols)
        part = lax.dot_general(
            og_s[:, columns], act_s[...], (((0,), (0,)), ((), ())), preferred_element_type=F32
        )
        wgt_s[i] = part.reshape(ny, 2, quarter, width)
        return carry

    lax.fori_loop(0, nz // 2, grad_step, 0)
    gather_round(4)
    lax.fori_loop(nz // 2, nz, grad_step, 0)

    hops, last = {}, {}

    def parts(h):
        return min(4, size(h, 1))

    def shifts(h, c):
        n = size(h, 1)
        order = sorted(range(n), key=lambda d: (-near(d, n), d))
        return order[c * n // parts(h) : (c + 1) * n // parts(h)]

    def term(h, shift, dest):
        q = lax.rem(place(h, 1) + shift, size(h, 1))
        return wgt_s[(*cell(h, q, dest), h)]

    def reduce_depth(h, c, sign):
        n = size(h, 2)
        return n // 2 if (c % 2 == 0) == (sign > 0) else n // 2 - 1

    def reduce_round(j):
        for c in range(4):
            for h in range(2):
                if c >= parts(h):
                    continue
                n = size(h, 2)
                part = pl.ds(0, size(h, 1) // parts(h))
                for i, sign in enumerate((1, -1)):
                    depth = reduce_depth(h, c, sign)
                    k = j - (n // 2 - depth)
                    if k < 1 or k > depth:
                        continue
                    dest = lax.rem(place(h, 2) + sign * (depth - k + 1) + n, n)
                    if k > 1:
                        hops[h, c, sign, k - 1].wait_recv()
                    for j_at, shift in enumerate(shifts(h, c)):
                        value = term(h, shift, dest)
                        if k > 1:
                            value = value + rs_r[h, c, i, k - 2, j_at].astype(F32)
                        rs_s[h, c, i, k - 1, j_at] = value.astype(BF16)
                    hops[h, c, sign, k] = send(
                        rs_s.at[h, c, i, k - 1, part],
                        rs_r.at[h, c, i, k - 1, part],
                        a2_rs.at[h, 2 * c + (k - 1) // 2, i, (k - 1) % 2],
                        along(h, 2, sign),
                    )

    def reduce_finish():
        for c in range(4):
            for h in range(2):
                if c >= parts(h):
                    continue
                for i, sign in enumerate((1, -1)):
                    if reduce_depth(h, c, sign):
                        hops[h, c, sign, reduce_depth(h, c, sign)].wait_recv()
                for j_at, shift in enumerate(shifts(h, c)):
                    value = term(h, shift, place(h, 2))
                    for i, sign in enumerate((1, -1)):
                        if reduce_depth(h, c, sign):
                            value = value + rs_r[h, c, i, reduce_depth(h, c, sign) - 1, j_at].astype(F32)
                    if shift == 0:
                        wgt_s[z, y, h] = value
                        continue
                    q_s[h, shift] = value.astype(BF16)
                    last[h, shift] = send(
                        q_s.at[h, shift], q_r.at[h, shift], r2_rs.at[h, shift], along(h, 1, shift)
                    )

    def reduce_end():
        for h in range(2):
            value = wgt_s[z, y, h]
            for d in range(1, size(h, 1)):
                last[h, d].wait_recv()
                value = value + q_r[h, d].astype(F32)
            wg_ref[h] = value

    for r in range(5, rounds - 1):
        gather_round(r)
    reduce_round(1)
    gather_round(rounds - 1)

    def product_step(i, carry):
        columns = pl.ds(pl.multiple_of(i * block_cols, 128), block_cols)
        part = jnp.dot(
            og_s[:, columns], wt_s[i].reshape(block_cols, width), preferred_element_type=F32
        )
        ag_s[...] = ag_s[...] + part
        return carry

    ag_s[...] = jnp.zeros_like(ag_s)
    lax.fori_loop(0, nz, product_step, 0)
    reduce_round(2)

    def pre_step(i, carry):
        gain_sum, bias_sum = carry
        here = pl.ds(pl.multiple_of(i * chunk, 8), chunk)
        normed = conv_s[here, :]
        pre = normed * gain_ref[...] + bias_ref[...]
        gate = jax.nn.sigmoid(pre)
        pre_grad = ag_s[here, :] * gate * (1.0 + pre * (1.0 - gate))
        gain_sum = gain_sum + jnp.sum((pre_grad * normed).reshape(chunk // 8, 8, width), axis=0)
        bias_sum = bias_sum + jnp.sum(pre_grad.reshape(chunk // 8, 8, width), axis=0)
        normed_grad = pre_grad * gain_ref[...]
        ag_s[here, :] = normed_grad
        s1_s[here, :] = fold(normed_grad)
        s2_s[here, :] = fold(normed_grad * normed)
        return gain_sum, bias_sum

    none = jnp.zeros((8, width), F32)
    gain_sum, bias_sum = lax.fori_loop(0, steps, pre_step, (none, none))
    gain_row = jnp.sum(gain_sum, axis=0, keepdims=True)
    bias_row = jnp.sum(bias_sum, axis=0, keepdims=True)
    sums = row_sums(1)
    reduce_round(3)
    total = gathered_sums(1, sums)
    b1_s[...] = down_rows(total[0:1])
    b2_s[...] = down_rows(total[1:2])

    def conv_grad_step(i, carry):
        base = pl.multiple_of(i * chunk, 8)
        here = pl.ds(base, chunk)
        value = wide(ib_s[here, :]) * (
            ag_s[here, :] - wide(b1_s[here, :]) - conv_s[here, :] * wide(b2_s[here, :])
        )
        cgpad[pl.ds(pl.multiple_of(base + EDGE, 8), chunk), :] = value
        return carry

    lax.fori_loop(0, steps, conv_grad_step, 0)
    back = [
        send(cgpad.at[pl.ds(rows, EDGE)], cg_recv.at[0], halo_rs.at[2], right_dev),
        send(cgpad.at[pl.ds(EDGE, EDGE)], cg_recv.at[1], halo_rs.at[3], left_dev),
    ]

    tacc[...] = jnp.zeros_like(tacc)

    def tap_step(i, carry):
        base = i * chunk
        value = cgpad[pl.ds(base + EDGE, chunk), :]
        for k in range(span):
            term = value * mpad[pl.ds(base + k + 1, chunk), :]
            tacc[k] = tacc[k] + jnp.sum(term.reshape(chunk // 8, 8, width), axis=0)
        return carry

    for i in range(steps):
        tap_step(i, 0)
    own_small = jnp.concatenate(
        [jnp.sum(tacc[...], axis=1), gain_row, bias_row, jnp.zeros((small_ref.shape[0] - span - 2, width), F32)],
        axis=0,
    )
    small_ref[...] = own_small

    def small_send(phase):
        copies = {}
        for h in range(2):
            ar_s[phase - 1, h] = small_ref[:, h * lanes : (h + 1) * lanes].astype(BF16)
        todo = [(-near(d, size(h, phase)), d, h) for h in range(2) for d in range(1, size(h, phase))]
        for _, d, h in sorted(todo):
            copies[h, d] = send(
                ar_s.at[phase - 1, h],
                ar_r.at[phase - 1, h, d],
                ar_rs.at[phase - 1, h, d],
                along(h, phase, d),
            )
        return copies

    def small_add(phase, copies):
        for h in range(2):
            value = ar_s[phase - 1, h].astype(F32)
            for d in range(1, size(h, phase)):
                copies[h, d].wait_recv()
                value = value + ar_r[phase - 1, h, d].astype(F32)
            small_ref[:, h * lanes : (h + 1) * lanes] = value

    small_1 = small_send(1)
    reduce_round(4)

    back[0].wait_recv()
    back[1].wait_recv()
    cgpad[:EDGE] = jnp.where(s == 0, 0.0, cg_recv[0])
    cgpad[EDGE + rows :] = jnp.where(s == count - 1, 0.0, cg_recv[1])

    def mixed_step(i, carry):
        base = i * chunk
        total = jnp.zeros((chunk, width), F32)
        for k in range(span):
            total = total + taps_ref[k : k + 1, :] * cgpad[pl.ds(base + span - k, chunk), :]
        ag_s[pl.ds(base, chunk), :] = total
        return carry

    for i in range(steps):
        mixed_step(i, 0)
    reduce_finish()
    small_add(1, small_1)
    small_2 = small_send(2)
    scaled = ag_s[...] * sig_s[...]
    v_s[...] = scaled.astype(BF16)
    g_s[...] = (scaled * vf_s[...] * (1.0 - sig_s[...])).astype(BF16)
    store_v = pltpu.make_async_copy(v_s, vg_hbm, local_sem.at[0])
    store_g = pltpu.make_async_copy(g_s, gg_hbm, local_sem.at[1])
    store_v.start()
    store_g.start()
    reduce_end()
    small_add(2, small_2)
    store_v.wait()
    store_g.wait()
    for copy in pending[-slots:]:
        copy.wait_send()


def finish(span, vg_ref, gg_ref, small_ref, wg_ref, vg_out, gg_out, tap_out, gain_out, bias_out, wg_out):
    vg_out[...] = vg_ref[...]
    gg_out[...] = gg_ref[...]
    wg_out[...] = wg_ref[...]
    tap_out[...] = small_ref[:span]
    gain_out[...] = small_ref[span : span + 1]
    bias_out[...] = small_ref[span + 1 : span + 2]


def on_device(sizes, value_in, gate_in, taps, norm_gain, norm_bias, proj_weight, out_grad):
    nz, ny, nt = sizes
    rows, width = value_in.shape
    span = taps.shape[0]
    n_col = proj_weight.shape[1]
    quarter = n_col // 2
    columns = out_grad.shape[1]
    lanes = width // 2
    chunk = next(c for c in (72, 24, 8) if rows % c == 0)
    padded_rows = (rows + 127) // 128 * 128
    small_rows = (span + 2 + 7) // 8 * 8
    n_max = max(nz, ny)
    n_half = n_max // 2
    dma = pltpu.SemaphoreType.DMA
    vmem = pl.BlockSpec(memory_space=pltpu.VMEM)
    hbm = pl.BlockSpec(memory_space=pltpu.HBM)
    cfg = (nz, ny, nt, rows, width, span, chunk)
    vg, gg, small, wg = pl.pallas_call(
        functools.partial(kernel, cfg),
        out_shape=(
            jax.ShapeDtypeStruct((rows, width), BF16),
            jax.ShapeDtypeStruct((rows, width), BF16),
            jax.ShapeDtypeStruct((small_rows, width), F32),
            jax.ShapeDtypeStruct((2, quarter, width), F32),
        ),
        in_specs=[hbm] * 7,
        out_specs=(hbm, hbm, vmem, vmem),
        scratch_shapes=[
            pltpu.VMEM((rows, width), BF16),
            pltpu.VMEM((rows, width), BF16),
            pltpu.VMEM((rows, columns), BF16),
            pltpu.VMEM((span, width), F32),
            pltpu.VMEM((1, width), F32),
            pltpu.VMEM((1, width), F32),
            pltpu.VMEM((rows, width), F32),
            pltpu.VMEM((rows, width), F32),
            pltpu.VMEM((rows + 2 * EDGE, width), F32),
            pltpu.VMEM((rows, width), F32),
            pltpu.VMEM((padded_rows, lanes), F32),
            pltpu.VMEM((padded_rows, lanes), F32),
            pltpu.VMEM((padded_rows, lanes), F32),
            pltpu.VMEM((padded_rows, lanes), F32),
            pltpu.VMEM((padded_rows, lanes), F32),
            pltpu.VMEM((rows, width), F32),
            pltpu.VMEM((rows, width), BF16),
            pltpu.VMEM((rows, width), F32),
            pltpu.VMEM((rows + 2 * EDGE, width), F32),
            pltpu.VMEM((span, 8, width), F32),
            pltpu.VMEM((2, EDGE, width), BF16),
            pltpu.VMEM((2, EDGE, width), BF16),
            pltpu.VMEM((2, EDGE, width), F32),
            pltpu.VMEM((2, 2, padded_rows), F32),
            pltpu.VMEM((2, nt, 2, padded_rows), F32),
            pltpu.VMEM((nz, ny, 2, quarter, width), BF16),
            pltpu.VMEM((nz, ny, 2, quarter, width), F32),
            pltpu.VMEM((2, 4, 2, n_half, max(1, n_max // 4), quarter, width), BF16),
            pltpu.VMEM((2, 4, 2, n_half, max(1, n_max // 4), quarter, width), BF16),
            pltpu.VMEM((2, n_max, quarter, width), BF16),
            pltpu.VMEM((2, n_max, quarter, width), BF16),
            pltpu.VMEM((2, 2, small_rows, lanes), BF16),
            pltpu.VMEM((2, 2, n_max, small_rows, lanes), BF16),
            dma((7,)),
            dma((40,)),
            dma((4,)),
            dma((2, nt)),
            dma((2, n_max)),
            dma((2, n_max, 2, n_half)),
            dma((2, n_max)),
            dma((2, 2, n_max)),
        ],
        compiler_params=pltpu.CompilerParams(
            collective_id=0, has_side_effects=True, vmem_limit_bytes=60 * 1024 * 1024
        ),
        name="step",
    )(
        value_in,
        gate_in,
        taps,
        norm_gain[None, :],
        norm_bias[None, :],
        proj_weight.T.reshape(2, quarter, width),
        out_grad,
    )
    vg, gg, tap, gain, bias, wg = pl.pallas_call(
        functools.partial(finish, span),
        out_shape=(
            jax.ShapeDtypeStruct((rows, width), BF16),
            jax.ShapeDtypeStruct((rows, width), BF16),
            jax.ShapeDtypeStruct((span, width), F32),
            jax.ShapeDtypeStruct((1, width), F32),
            jax.ShapeDtypeStruct((1, width), F32),
            jax.ShapeDtypeStruct((2, quarter, width), F32),
        ),
        in_specs=[vmem] * 4,
        out_specs=(vmem,) * 6,
        compiler_params=pltpu.CompilerParams(vmem_limit_bytes=60 * 1024 * 1024),
        name="finish",
    )(vg, gg, small, wg)
    return (vg, gg, tap, gain[0], bias[0], jnp.transpose(wg.reshape(n_col, width)))


def solution(mesh):
    tp = mesh.shape["tp"]
    ny = 8 if mesh.shape["sp"] % 8 == 0 else 2
    nz = mesh.shape["sp"] // ny
    finer = Mesh(mesh.devices.reshape(nz, ny, tp), (*SP, "tp"))
    in_specs = (P(SP, "tp"), P(SP, "tp"), P(None, "tp"), P("tp"), P("tp"), P("tp", SP), P(SP, None))
    out_specs = (P(SP, "tp"), P(SP, "tp"), P(None, "tp"), P("tp"), P("tp"), P("tp", SP))
    return jax.shard_map(
        functools.partial(on_device, (nz, ny, tp)),
        mesh=finer,
        in_specs=in_specs,
        out_specs=out_specs,
        check_vma=False,
    )
```

```python
import functools

import jax
import jax.numpy as jnp
from jax import lax
from jax.experimental import pallas as pl
from jax.experimental.pallas import tpu as pltpu
from jax.sharding import Mesh
from jax.sharding import PartitionSpec as P

SP = ("sp_0", "sp_1")
MESH = pl.DeviceIdType.MESH
EPS = 1e-06
F32 = jnp.float32
BF16 = jnp.bfloat16
EDGE = 16


def kernel(
    cfg,
    v_hbm,
    g_hbm,
    taps_hbm,
    gain_hbm,
    bias_hbm,
    w_hbm,
    og_hbm,
    vg_hbm,
    gg_hbm,
    small_ref,
    wg_ref,
    v_s,
    g_s,
    og_s,
    taps_ref,
    gain_ref,
    bias_ref,
    vf_s,
    sig_s,
    mpad,
    conv_s,
    s1_s,
    s2_s,
    b1_s,
    b2_s,
    ib_s,
    act_f,
    act_s,
    ag_s,
    cgpad,
    tacc,
    halo_send,
    halo_recv,
    cg_recv,
    st_send,
    st_recv,
    wt_s,
    wgt_s,
    rs_s,
    rs_r,
    q_s,
    q_r,
    ar_s,
    ar_r,
    local_sem,
    send_sem,
    halo_rs,
    st_rs,
    a1_rs,
    a2_rs,
    r2_rs,
    ar_rs,
):
    nz, ny, nt, rows, width, span, chunk = cfg
    z, y, t = lax.axis_index("sp_0"), lax.axis_index("sp_1"), lax.axis_index("tp")
    count = nz * ny
    s = z * ny + y
    lanes = width // 2
    channels = width * nt
    steps = rows // chunk
    padded_rows = s1_s.shape[0]
    quarter = w_hbm.shape[1]
    n_col = 2 * quarter

    def at(zz, yy, tt):
        return (zz, yy, tt)

    def along(h, phase, shift):
        on_y = (h == 0) == (phase == 1)
        if on_y:
            return at(z, lax.rem(y + shift + ny, ny), t)
        return at(lax.rem(z + shift + nz, nz), y, t)

    def size(h, phase):
        return ny if (h == 0) == (phase == 1) else nz

    def place(h, phase):
        return y if (h == 0) == (phase == 1) else z

    def cell(h, a, b):
        return (b, a) if h == 0 else (a, b)

    pending = []
    slots = send_sem.shape[0]

    def send(src, dst, rsem, dev):
        slot = len(pending) % slots
        if len(pending) >= slots:
            pending[-slots].wait_send()
        copy = pltpu.make_async_remote_copy(
            src_ref=src,
            dst_ref=dst,
            send_sem=send_sem.at[slot],
            recv_sem=rsem,
            device_id=dev,
            device_id_type=MESH,
        )
        copy.start()
        pending.append(copy)
        return copy

    load_v = pltpu.make_async_copy(v_hbm, v_s, local_sem.at[0])
    load_g = pltpu.make_async_copy(g_hbm, g_s, local_sem.at[1])
    load_og = pltpu.make_async_copy(og_hbm, og_s, local_sem.at[2])
    load_w = pltpu.make_async_copy(w_hbm, wt_s.at[z, y], local_sem.at[3])
    load_taps = pltpu.make_async_copy(taps_hbm, taps_ref, local_sem.at[4])
    load_gain = pltpu.make_async_copy(gain_hbm, gain_ref, local_sem.at[5])
    load_bias = pltpu.make_async_copy(bias_hbm, bias_ref, local_sem.at[6])
    for load in (load_g, load_v, load_w, load_taps, load_gain, load_bias, load_og):
        load.start()

    right = lax.rem(s + 1, count)
    left = lax.rem(s + count - 1, count)
    right_dev = at(right // ny, lax.rem(right, ny), t)
    left_dev = at(left // ny, lax.rem(left, ny), t)
    barrier = pltpu.get_barrier_semaphore()
    peers = [right_dev, left_dev]
    peers += [at(z, lax.rem(y + d, ny), t) for d in range(1, ny)]
    peers += [at(lax.rem(z + d, nz), y, t) for d in range(1, nz)]
    peers += [at(z, y, lax.rem(t + d, nt)) for d in range(1, nt)]
    for dev in peers:
        pl.semaphore_signal(barrier, inc=1, device_id=dev, device_id_type=MESH)

    load_g.wait()
    load_v.wait()
    sig = jax.nn.sigmoid(g_s[...].astype(F32))
    sig_s[...] = sig
    vf = v_s[...].astype(F32)
    vf_s[...] = vf
    mixed = (vf * sig).astype(BF16)
    halo_send[0] = mixed[rows - EDGE :]
    halo_send[1] = mixed[:EDGE]
    mpad[EDGE : EDGE + rows] = mixed.astype(F32)

    for load in (load_w, load_taps, load_gain, load_bias):
        load.wait()
    pl.semaphore_wait(barrier, len(peers))

    halo = [
        send(halo_send.at[0], halo_recv.at[0], halo_rs.at[0], right_dev),
        send(halo_send.at[1], halo_recv.at[1], halo_rs.at[1], left_dev),
    ]

    first, ring = {}, {}

    def near(d, n):
        return min(d, n - d)

    def ring_depth(h, d, sign):
        n = size(h, 2)
        even = d % 2 == 0
        return n // 2 if even == (sign > 0) else n // 2 - 1

    def forward(h, d, sign, k):
        a = lax.rem(place(h, 1) - d + size(h, 1), size(h, 1))
        n = size(h, 2)
        b = lax.rem(place(h, 2) - sign * (k - 1) + n, n)
        block = wt_s.at[(*cell(h, a, b), h)]
        i = 0 if sign > 0 else 1
        ring[h, d, sign, k] = send(
            block, block, a2_rs.at[h, d, i * (n // 2 - 1) + k - 1 if k < n // 2 else n - 2], along(h, 2, sign)
        )

    def gather_start():
        for h in range(2):
            for sign in (1, -1):
                if ring_depth(h, 0, sign) >= 1:
                    forward(h, 0, sign, 1)
        todo = [(near(d, size(h, 1)), d, h) for h in range(2) for d in range(1, size(h, 1))]
        for _, d, h in sorted(todo):
            block = wt_s.at[(*cell(h, place(h, 1), place(h, 2)), h)]
            first[h, d] = send(block, block, a1_rs.at[h, d - 1], along(h, 1, d))

    def gather_round(r, low=0, high=99):
        todo = []
        for h in range(2):
            n = size(h, 1)
            for d in range(n):
                k = r - min(near(d, n), 1) + 1
                if (d == 0 and k == 1) or k < 1 or k > size(h, 2) // 2 + 1 or not low <= near(d, n) <= high:
                    continue
                todo.append((near(d, n), d, h, k))
        for _, d, h, k in sorted(todo):
            if k == 1:
                first[h, d].wait_recv()
            for sign in (1, -1):
                depth = ring_depth(h, d, sign)
                if 1 <= k - 1 <= depth:
                    ring[h, d, sign, k - 1].wait_recv()
                if k <= depth:
                    forward(h, d, sign, k)

    rounds = max(size(h, 2) // 2 + 2 for h in range(2))
    gather_start()
    gather_round(1, 0, 2)

    halo[0].wait_recv()
    halo[1].wait_recv()
    gather_round(1, 3)
    mpad[:EDGE] = jnp.where(s == 0, 0.0, halo_recv[0].astype(F32))
    mpad[EDGE + rows :] = jnp.where(s == count - 1, 0.0, halo_recv[1].astype(F32))

    def fold(x):
        return x[:, :lanes] + x[:, lanes:]

    def wide(x):
        return jnp.concatenate([x, x], axis=1)

    def conv_step(i, carry):
        base = i * chunk
        total = jnp.zeros((chunk, width), F32)
        for k in range(span):
            total = total + taps_ref[k : k + 1, :] * mpad[pl.ds(base + k + 1, chunk), :]
        conv_s[pl.ds(base, chunk), :] = total
        s1_s[pl.ds(base, chunk), :] = fold(total)
        s2_s[pl.ds(base, chunk), :] = fold(total * total)
        return carry

    for i in range(steps):
        conv_step(i, 0)

    def row_sums(which):
        a = jnp.sum(jnp.transpose(s1_s[...]), axis=0, keepdims=True)
        b = jnp.sum(jnp.transpose(s2_s[...]), axis=0, keepdims=True)
        both = jnp.concatenate([a, b], axis=0)
        st_send[which] = both
        copies = []
        for d in range(1, nt):
            copies.append(
                send(
                    st_send.at[which],
                    st_recv.at[which, d],
                    st_rs.at[which, d - 1],
                    at(z, y, lax.rem(t + d, nt)),
                )
            )
        return copies

    def gathered_sums(which, copies):
        total = st_send[which]
        for d in range(1, nt):
            copies[d - 1].wait_recv()
            total = total + st_recv[which, d]
        return total / channels

    def down_rows(row):
        return jnp.transpose(jnp.broadcast_to(row, (lanes, padded_rows)))

    sums = row_sums(0)
    gather_round(2)
    gather_round(3)
    total = gathered_sums(0, sums)
    mean = total[0:1]
    inv = lax.rsqrt(total[1:2] - mean * mean + EPS)
    b1_s[...] = down_rows(mean)
    ib_s[...] = down_rows(inv)

    def act_step(i, carry):
        here = pl.ds(pl.multiple_of(i * chunk, 8), chunk)
        normed = (conv_s[here, :] - wide(b1_s[here, :])) * wide(ib_s[here, :])
        conv_s[here, :] = normed
        pre = normed * gain_ref[...] + bias_ref[...]
        act_f[here, :] = pre * jax.nn.sigmoid(pre)
        return carry

    lax.fori_loop(0, steps, act_step, 0)
    act_s[...] = act_f[...].astype(BF16)
    load_og.wait()

    block_cols = ny * n_col

    def grad_step(i, carry):
        columns = pl.ds(pl.multiple_of(i * block_cols, 128), block_cols)
        part = lax.dot_general(
            og_s[:, columns], act_s[...], (((0,), (0,)), ((), ())), preferred_element_type=F32
        )
        wgt_s[i] = part.reshape(ny, 2, quarter, width)
        return carry

    lax.fori_loop(0, nz // 2, grad_step, 0)
    gather_round(4)
    lax.fori_loop(nz // 2, nz, grad_step, 0)

    hops, last = {}, {}

    def parts(h):
        return min(4, size(h, 1))

    def shifts(h, c):
        n = size(h, 1)
        order = sorted(range(n), key=lambda d: (-near(d, n), d))
        return order[c * n // parts(h) : (c + 1) * n // parts(h)]

    def term(h, shift, dest):
        q = lax.rem(place(h, 1) + shift, size(h, 1))
        return wgt_s[(*cell(h, q, dest), h)]

    def reduce_depth(h, c, sign):
        n = size(h, 2)
        return n // 2 if (c % 2 == 0) == (sign > 0) else n // 2 - 1

    def reduce_round(j):
        for c in range(4):
            for h in range(2):
                if c >= parts(h):
                    continue
                n = size(h, 2)
                part = pl.ds(0, size(h, 1) // parts(h))
                for i, sign in enumerate((1, -1)):
                    depth = reduce_depth(h, c, sign)
                    k = j - (n // 2 - depth)
                    if k < 1 or k > depth:
                        continue
                    dest = lax.rem(place(h, 2) + sign * (depth - k + 1) + n, n)
                    if k > 1:
                        hops[h, c, sign, k - 1].wait_recv()
                    for j_at, shift in enumerate(shifts(h, c)):
                        value = term(h, shift, dest)
                        if k > 1:
                            value = value + rs_r[h, c, i, k - 2, j_at].astype(F32)
                        rs_s[h, c, i, k - 1, j_at] = value.astype(BF16)
                    hops[h, c, sign, k] = send(
                        rs_s.at[h, c, i, k - 1, part],
                        rs_r.at[h, c, i, k - 1, part],
                        a2_rs.at[h, 2 * c + (k - 1) // 2, i * (n // 2 - 1) + (k - 1) % 2],
                        along(h, 2, sign),
                    )

    def reduce_finish(chunks):
        for c in chunks:
            for h in range(2):
                if c >= parts(h):
                    continue
                for i, sign in enumerate((1, -1)):
                    if reduce_depth(h, c, sign):
                        hops[h, c, sign, reduce_depth(h, c, sign)].wait_recv()
                for j_at, shift in enumerate(shifts(h, c)):
                    value = term(h, shift, place(h, 2))
                    for i, sign in enumerate((1, -1)):
                        if reduce_depth(h, c, sign):
                            value = value + rs_r[h, c, i, reduce_depth(h, c, sign) - 1, j_at].astype(F32)
                    if shift == 0:
                        wgt_s[z, y, h] = value
                        continue
                    q_s[h, shift] = value.astype(BF16)
                    last[h, shift] = send(
                        q_s.at[h, shift], q_r.at[h, shift], r2_rs.at[h, shift - 1], along(h, 1, shift)
                    )

    def reduce_end():
        for h in range(2):
            value = wgt_s[z, y, h]
            for d in range(1, size(h, 1)):
                last[h, d].wait_recv()
                value = value + q_r[h, d].astype(F32)
            wg_ref[h] = value

    for r in range(5, rounds - 1):
        gather_round(r)
    reduce_round(1)
    gather_round(rounds - 1)

    def product_step(i, carry):
        columns = pl.ds(pl.multiple_of(i * block_cols, 128), block_cols)
        part = jnp.dot(
            og_s[:, columns], wt_s[i].reshape(block_cols, width), preferred_element_type=F32
        )
        ag_s[...] = ag_s[...] + part
        return carry

    ag_s[...] = jnp.zeros_like(ag_s)
    lax.fori_loop(0, nz // 2, product_step, 0)
    reduce_round(2)
    lax.fori_loop(nz // 2, nz, product_step, 0)

    def pre_step(i, carry):
        gain_sum, bias_sum = carry
        here = pl.ds(pl.multiple_of(i * chunk, 8), chunk)
        normed = conv_s[here, :]
        pre = normed * gain_ref[...] + bias_ref[...]
        gate = jax.nn.sigmoid(pre)
        pre_grad = ag_s[here, :] * gate * (1.0 + pre * (1.0 - gate))
        gain_sum = gain_sum + jnp.sum((pre_grad * normed).reshape(chunk // 8, 8, width), axis=0)
        bias_sum = bias_sum + jnp.sum(pre_grad.reshape(chunk // 8, 8, width), axis=0)
        normed_grad = pre_grad * gain_ref[...]
        ag_s[here, :] = normed_grad
        s1_s[here, :] = fold(normed_grad)
        s2_s[here, :] = fold(normed_grad * normed)
        return gain_sum, bias_sum

    none = jnp.zeros((8, width), F32)
    gain_sum, bias_sum = lax.fori_loop(0, steps, pre_step, (none, none))
    gain_row = jnp.sum(gain_sum, axis=0, keepdims=True)
    bias_row = jnp.sum(bias_sum, axis=0, keepdims=True)
    sums = row_sums(1)
    reduce_round(3)
    total = gathered_sums(1, sums)
    b1_s[...] = down_rows(total[0:1])
    b2_s[...] = down_rows(total[1:2])

    def conv_grad_step(i, carry):
        base = pl.multiple_of(i * chunk, 8)
        here = pl.ds(base, chunk)
        value = wide(ib_s[here, :]) * (
            ag_s[here, :] - wide(b1_s[here, :]) - conv_s[here, :] * wide(b2_s[here, :])
        )
        cgpad[pl.ds(pl.multiple_of(base + EDGE, 8), chunk), :] = value
        return carry

    lax.fori_loop(0, steps, conv_grad_step, 0)
    back = [
        send(cgpad.at[pl.ds(rows, EDGE)], cg_recv.at[0], halo_rs.at[2], right_dev),
        send(cgpad.at[pl.ds(EDGE, EDGE)], cg_recv.at[1], halo_rs.at[3], left_dev),
    ]

    tacc[...] = jnp.zeros_like(tacc)

    def tap_step(i, carry):
        base = i * chunk
        value = cgpad[pl.ds(base + EDGE, chunk), :]
        for k in range(span):
            term = value * mpad[pl.ds(base + k + 1, chunk), :]
            tacc[k] = tacc[k] + jnp.sum(term.reshape(chunk // 8, 8, width), axis=0)
        return carry

    for i in range(steps):
        tap_step(i, 0)
    own_small = jnp.concatenate(
        [jnp.sum(tacc[...], axis=1), gain_row, bias_row, jnp.zeros((small_ref.shape[0] - span - 2, width), F32)],
        axis=0,
    )
    small_ref[...] = own_small

    def small_send(phase):
        copies = {}
        for h in range(2):
            ar_s[phase - 1, h] = small_ref[:, h * lanes : (h + 1) * lanes].astype(BF16)
        todo = [(-near(d, size(h, phase)), d, h) for h in range(2) for d in range(1, size(h, phase))]
        for _, d, h in sorted(todo):
            copies[h, d] = send(
                ar_s.at[phase - 1, h],
                ar_r.at[phase - 1, h, d],
                ar_rs.at[phase - 1, h, d - 1],
                along(h, phase, d),
            )
        return copies

    def small_add(phase, copies):
        for h in range(2):
            value = ar_s[phase - 1, h].astype(F32)
            for d in range(1, size(h, phase)):
                copies[h, d].wait_recv()
                value = value + ar_r[phase - 1, h, d].astype(F32)
            small_ref[:, h * lanes : (h + 1) * lanes] = value

    small_1 = small_send(1)
    reduce_round(4)

    back[0].wait_recv()
    back[1].wait_recv()
    cgpad[:EDGE] = jnp.where(s == 0, 0.0, cg_recv[0])
    cgpad[EDGE + rows :] = jnp.where(s == count - 1, 0.0, cg_recv[1])

    def mixed_step(i, carry):
        base = i * chunk
        total = jnp.zeros((chunk, width), F32)
        for k in range(span):
            total = total + taps_ref[k : k + 1, :] * cgpad[pl.ds(base + span - k, chunk), :]
        ag_s[pl.ds(base, chunk), :] = total
        return carry

    for i in range(steps):
        mixed_step(i, 0)
    reduce_finish(range(4))
    small_add(1, small_1)
    small_2 = small_send(2)
    scaled = ag_s[...] * sig_s[...]
    v_s[...] = scaled.astype(BF16)
    g_s[...] = (scaled * vf_s[...] * (1.0 - sig_s[...])).astype(BF16)
    store_v = pltpu.make_async_copy(v_s, vg_hbm, local_sem.at[0])
    store_g = pltpu.make_async_copy(g_s, gg_hbm, local_sem.at[1])
    store_v.start()
    store_g.start()
    reduce_end()
    small_add(2, small_2)
    store_v.wait()
    store_g.wait()
    for copy in pending[-slots:]:
        copy.wait_send()


def finish(span, vg_ref, gg_ref, small_ref, wg_ref, vg_out, gg_out, tap_out, gain_out, bias_out, wg_out):
    vg_out[...] = vg_ref[...]
    gg_out[...] = gg_ref[...]
    wg_out[...] = wg_ref[...]
    tap_out[...] = small_ref[:span]
    gain_out[...] = small_ref[span : span + 1]
    bias_out[...] = small_ref[span + 1 : span + 2]


def on_device(sizes, value_in, gate_in, taps, norm_gain, norm_bias, proj_weight, out_grad):
    nz, ny, nt = sizes
    rows, width = value_in.shape
    span = taps.shape[0]
    n_col = proj_weight.shape[1]
    quarter = n_col // 2
    columns = out_grad.shape[1]
    lanes = width // 2
    chunk = next(c for c in (72, 24, 8) if rows % c == 0)
    padded_rows = (rows + 127) // 128 * 128
    small_rows = (span + 2 + 7) // 8 * 8
    n_max = max(nz, ny)
    n_half = n_max // 2
    dma = pltpu.SemaphoreType.DMA
    vmem = pl.BlockSpec(memory_space=pltpu.VMEM)
    hbm = pl.BlockSpec(memory_space=pltpu.HBM)
    cfg = (nz, ny, nt, rows, width, span, chunk)
    vg, gg, small, wg = pl.pallas_call(
        functools.partial(kernel, cfg),
        out_shape=(
            jax.ShapeDtypeStruct((rows, width), BF16),
            jax.ShapeDtypeStruct((rows, width), BF16),
            jax.ShapeDtypeStruct((small_rows, width), F32),
            jax.ShapeDtypeStruct((2, quarter, width), F32),
        ),
        in_specs=[hbm] * 7,
        out_specs=(hbm, hbm, vmem, vmem),
        scratch_shapes=[
            pltpu.VMEM((rows, width), BF16),
            pltpu.VMEM((rows, width), BF16),
            pltpu.VMEM((rows, columns), BF16),
            pltpu.VMEM((span, width), F32),
            pltpu.VMEM((1, width), F32),
            pltpu.VMEM((1, width), F32),
            pltpu.VMEM((rows, width), F32),
            pltpu.VMEM((rows, width), F32),
            pltpu.VMEM((rows + 2 * EDGE, width), F32),
            pltpu.VMEM((rows, width), F32),
            pltpu.VMEM((padded_rows, lanes), F32),
            pltpu.VMEM((padded_rows, lanes), F32),
            pltpu.VMEM((padded_rows, lanes), F32),
            pltpu.VMEM((padded_rows, lanes), F32),
            pltpu.VMEM((padded_rows, lanes), F32),
            pltpu.VMEM((rows, width), F32),
            pltpu.VMEM((rows, width), BF16),
            pltpu.VMEM((rows, width), F32),
            pltpu.VMEM((rows + 2 * EDGE, width), F32),
            pltpu.VMEM((span, 8, width), F32),
            pltpu.VMEM((2, EDGE, width), BF16),
            pltpu.VMEM((2, EDGE, width), BF16),
            pltpu.VMEM((2, EDGE, width), F32),
            pltpu.VMEM((2, 2, padded_rows), F32),
            pltpu.VMEM((2, nt, 2, padded_rows), F32),
            pltpu.VMEM((nz, ny, 2, quarter, width), BF16),
            pltpu.VMEM((nz, ny, 2, quarter, width), F32),
            pltpu.VMEM((2, 4, 2, n_half, max(1, n_max // 4), quarter, width), BF16),
            pltpu.VMEM((2, 4, 2, n_half, max(1, n_max // 4), quarter, width), BF16),
            pltpu.VMEM((2, n_max, quarter, width), BF16),
            pltpu.VMEM((2, n_max, quarter, width), BF16),
            pltpu.VMEM((2, 2, small_rows, lanes), BF16),
            pltpu.VMEM((2, 2, n_max, small_rows, lanes), BF16),
            dma((7,)),
            dma((32,)),
            dma((4,)),
            dma((2, nt - 1)),
            dma((2, n_max - 1)),
            dma((2, n_max, n_max - 1)),
            dma((2, n_max - 1)),
            dma((2, 2, n_max - 1)),
        ],
        compiler_params=pltpu.CompilerParams(
            collective_id=0, has_side_effects=True, vmem_limit_bytes=60 * 1024 * 1024
        ),
        name="step",
    )(
        value_in,
        gate_in,
        taps,
        norm_gain[None, :],
        norm_bias[None, :],
        proj_weight.T.reshape(2, quarter, width),
        out_grad,
    )
    vg, gg, tap, gain, bias, wg = pl.pallas_call(
        functools.partial(finish, span),
        out_shape=(
            jax.ShapeDtypeStruct((rows, width), BF16),
            jax.ShapeDtypeStruct((rows, width), BF16),
            jax.ShapeDtypeStruct((span, width), F32),
            jax.ShapeDtypeStruct((1, width), F32),
            jax.ShapeDtypeStruct((1, width), F32),
            jax.ShapeDtypeStruct((2, quarter, width), F32),
        ),
        in_specs=[vmem] * 4,
        out_specs=(vmem,) * 6,
        compiler_params=pltpu.CompilerParams(vmem_limit_bytes=60 * 1024 * 1024),
        name="finish",
    )(vg, gg, small, wg)
    return (vg, gg, tap, gain[0], bias[0], jnp.transpose(wg.reshape(n_col, width)))


def solution(mesh):
    tp = mesh.shape["tp"]
    ny = 8 if mesh.shape["sp"] % 8 == 0 else 2
    nz = mesh.shape["sp"] // ny
    finer = Mesh(mesh.devices.reshape(nz, ny, tp), (*SP, "tp"))
    in_specs = (P(SP, "tp"), P(SP, "tp"), P(None, "tp"), P("tp"), P("tp"), P("tp", SP), P(SP, None))
    out_specs = (P(SP, "tp"), P(SP, "tp"), P(None, "tp"), P("tp"), P("tp"), P("tp", SP))
    return jax.shard_map(
        functools.partial(on_device, (nz, ny, tp)),
        mesh=finer,
        in_specs=in_specs,
        out_specs=out_specs,
        check_vma=False,
    )
```

```python
import functools

import jax
import jax.numpy as jnp
from jax import lax
from jax.experimental import pallas as pl
from jax.experimental.pallas import tpu as pltpu
from jax.sharding import Mesh
from jax.sharding import PartitionSpec as P

SP = ("sp_0", "sp_1")
MESH = pl.DeviceIdType.MESH
EPS = 1e-06
F32 = jnp.float32
BF16 = jnp.bfloat16
EDGE = 16


def kernel(
    cfg,
    v_hbm,
    g_hbm,
    taps_hbm,
    gain_hbm,
    bias_hbm,
    w_hbm,
    og_hbm,
    vg_hbm,
    gg_hbm,
    small_ref,
    wg_ref,
    v_s,
    g_s,
    og_s,
    taps_ref,
    gain_ref,
    bias_ref,
    vf_s,
    sig_s,
    mpad,
    conv_s,
    s1_s,
    s2_s,
    b1_s,
    b2_s,
    ib_s,
    act_f,
    act_s,
    ag_s,
    cgpad,
    tacc,
    halo_send,
    halo_recv,
    cg_recv,
    st_send,
    st_recv,
    wt_s,
    wgt_s,
    rs_s,
    rs_r,
    q_s,
    q_r,
    ar_s,
    ar_r,
    local_sem,
    send_sem,
    halo_rs,
    st_rs,
    a1_rs,
    a2_rs,
    r2_rs,
    ar_rs,
):
    nz, ny, nt, rows, width, span, chunk = cfg
    z, y, t = lax.axis_index("sp_0"), lax.axis_index("sp_1"), lax.axis_index("tp")
    count = nz * ny
    s = z * ny + y
    lanes = width // 2
    channels = width * nt
    steps = rows // chunk
    padded_rows = s1_s.shape[0]
    quarter = w_hbm.shape[1]
    n_col = 2 * quarter

    def at(zz, yy, tt):
        return (zz, yy, tt)

    def along(h, phase, shift):
        on_y = (h == 0) == (phase == 1)
        if on_y:
            return at(z, lax.rem(y + shift + ny, ny), t)
        return at(lax.rem(z + shift + nz, nz), y, t)

    def size(h, phase):
        return ny if (h == 0) == (phase == 1) else nz

    def place(h, phase):
        return y if (h == 0) == (phase == 1) else z

    def cell(h, a, b):
        return (b, a) if h == 0 else (a, b)

    pending = []
    slots = send_sem.shape[0]

    def send(src, dst, rsem, dev):
        slot = len(pending) % slots
        if len(pending) >= slots:
            pending[-slots].wait_send()
        copy = pltpu.make_async_remote_copy(
            src_ref=src,
            dst_ref=dst,
            send_sem=send_sem.at[slot],
            recv_sem=rsem,
            device_id=dev,
            device_id_type=MESH,
        )
        copy.start()
        pending.append(copy)
        return copy

    load_v = pltpu.make_async_copy(v_hbm, v_s, local_sem.at[0])
    load_g = pltpu.make_async_copy(g_hbm, g_s, local_sem.at[1])
    load_og = pltpu.make_async_copy(og_hbm, og_s, local_sem.at[2])
    load_w = pltpu.make_async_copy(w_hbm, wt_s.at[z, y], local_sem.at[3])
    load_taps = pltpu.make_async_copy(taps_hbm, taps_ref, local_sem.at[4])
    load_gain = pltpu.make_async_copy(gain_hbm, gain_ref, local_sem.at[5])
    load_bias = pltpu.make_async_copy(bias_hbm, bias_ref, local_sem.at[6])
    for load in (load_g, load_v, load_w, load_taps, load_gain, load_bias, load_og):
        load.start()

    right = lax.rem(s + 1, count)
    left = lax.rem(s + count - 1, count)
    right_dev = at(right // ny, lax.rem(right, ny), t)
    left_dev = at(left // ny, lax.rem(left, ny), t)
    barrier = pltpu.get_barrier_semaphore()
    peers = [right_dev, left_dev]
    peers += [at(z, lax.rem(y + d, ny), t) for d in range(1, ny)]
    peers += [at(lax.rem(z + d, nz), y, t) for d in range(1, nz)]
    peers += [at(z, y, lax.rem(t + d, nt)) for d in range(1, nt)]
    for dev in peers:
        pl.semaphore_signal(barrier, inc=1, device_id=dev, device_id_type=MESH)

    load_g.wait()
    load_v.wait()
    sig = jax.nn.sigmoid(g_s[...].astype(F32))
    sig_s[...] = sig
    vf = v_s[...].astype(F32)
    vf_s[...] = vf
    mixed = (vf * sig).astype(BF16)
    halo_send[0] = mixed[rows - EDGE :]
    halo_send[1] = mixed[:EDGE]
    mpad[EDGE : EDGE + rows] = mixed.astype(F32)

    for load in (load_w, load_taps, load_gain, load_bias):
        load.wait()
    pl.semaphore_wait(barrier, len(peers))

    halo = [
        send(halo_send.at[0], halo_recv.at[0], halo_rs.at[0], right_dev),
        send(halo_send.at[1], halo_recv.at[1], halo_rs.at[1], left_dev),
    ]

    first, ring = {}, {}

    def near(d, n):
        return min(d, n - d)

    def ring_depth(h, d, sign):
        n = size(h, 2)
        even = d % 2 == 0
        return n // 2 if even == (sign > 0) else n // 2 - 1

    def forward(h, d, sign, k):
        a = lax.rem(place(h, 1) - d + size(h, 1), size(h, 1))
        n = size(h, 2)
        b = lax.rem(place(h, 2) - sign * (k - 1) + n, n)
        block = wt_s.at[(*cell(h, a, b), h)]
        i = 0 if sign > 0 else 1
        ring[h, d, sign, k] = send(
            block, block, a2_rs.at[h, d, i * (n // 2 - 1) + k - 1 if k < n // 2 else n - 2], along(h, 2, sign)
        )

    def gather_start():
        for h in range(2):
            for sign in (1, -1):
                if ring_depth(h, 0, sign) >= 1:
                    forward(h, 0, sign, 1)
        todo = [(near(d, size(h, 1)), d, h) for h in range(2) for d in range(1, size(h, 1))]
        for _, d, h in sorted(todo):
            block = wt_s.at[(*cell(h, place(h, 1), place(h, 2)), h)]
            first[h, d] = send(block, block, a1_rs.at[h, d - 1], along(h, 1, d))

    def gather_round(r, low=0, high=99):
        todo = []
        for h in range(2):
            n = size(h, 1)
            for d in range(n):
                k = r - min(near(d, n), 1) + 1
                if (d == 0 and k == 1) or k < 1 or k > size(h, 2) // 2 + 1 or not low <= near(d, n) <= high:
                    continue
                todo.append((near(d, n), d, h, k))
        for _, d, h, k in sorted(todo):
            if k == 1:
                first[h, d].wait_recv()
            for sign in (1, -1):
                depth = ring_depth(h, d, sign)
                if 1 <= k - 1 <= depth:
                    ring[h, d, sign, k - 1].wait_recv()
                if k <= depth:
                    forward(h, d, sign, k)

    rounds = max(size(h, 2) // 2 + 2 for h in range(2))
    gather_start()
    gather_round(1, 0, 2)

    halo[0].wait_recv()
    halo[1].wait_recv()
    gather_round(1, 3)
    mpad[:EDGE] = jnp.where(s == 0, 0.0, halo_recv[0].astype(F32))
    mpad[EDGE + rows :] = jnp.where(s == count - 1, 0.0, halo_recv[1].astype(F32))

    def fold(x):
        return x[:, :lanes] + x[:, lanes:]

    def wide(x):
        return jnp.concatenate([x, x], axis=1)

    def conv_step(i, carry):
        base = i * chunk
        total = jnp.zeros((chunk, width), F32)
        for k in range(span):
            total = total + taps_ref[k : k + 1, :] * mpad[pl.ds(base + k + 1, chunk), :]
        conv_s[pl.ds(base, chunk), :] = total
        s1_s[pl.ds(base, chunk), :] = fold(total)
        s2_s[pl.ds(base, chunk), :] = fold(total * total)
        return carry

    for i in range(steps):
        conv_step(i, 0)

    def row_sums(which):
        a = jnp.sum(jnp.transpose(s1_s[...]), axis=0, keepdims=True)
        b = jnp.sum(jnp.transpose(s2_s[...]), axis=0, keepdims=True)
        both = jnp.concatenate([a, b], axis=0)
        st_send[which] = both
        copies = []
        for d in range(1, nt):
            copies.append(
                send(
                    st_send.at[which],
                    st_recv.at[which, d],
                    st_rs.at[which, d - 1],
                    at(z, y, lax.rem(t + d, nt)),
                )
            )
        return copies

    def gathered_sums(which, copies):
        total = st_send[which]
        for d in range(1, nt):
            copies[d - 1].wait_recv()
            total = total + st_recv[which, d]
        return total / channels

    def down_rows(row):
        return jnp.transpose(jnp.broadcast_to(row, (lanes, padded_rows)))

    sums = row_sums(0)
    gather_round(2)
    gather_round(3)
    total = gathered_sums(0, sums)
    mean = total[0:1]
    inv = lax.rsqrt(total[1:2] - mean * mean + EPS)
    b1_s[...] = down_rows(mean)
    ib_s[...] = down_rows(inv)

    def act_step(i, carry):
        here = pl.ds(pl.multiple_of(i * chunk, 8), chunk)
        normed = (conv_s[here, :] - wide(b1_s[here, :])) * wide(ib_s[here, :])
        conv_s[here, :] = normed
        pre = normed * gain_ref[...] + bias_ref[...]
        act_f[here, :] = pre * jax.nn.sigmoid(pre)
        return carry

    lax.fori_loop(0, steps, act_step, 0)
    act_s[...] = act_f[...].astype(BF16)
    load_og.wait()

    block_cols = ny * n_col

    def grad_step(i, carry):
        columns = pl.ds(pl.multiple_of(i * block_cols, 128), block_cols)
        part = lax.dot_general(
            og_s[:, columns], act_s[...], (((0,), (0,)), ((), ())), preferred_element_type=F32
        )
        wgt_s[i] = part.reshape(ny, 2, quarter, width)
        return carry

    lax.fori_loop(0, nz // 2, grad_step, 0)
    gather_round(4)
    lax.fori_loop(nz // 2, nz, grad_step, 0)

    hops, last = {}, {}

    def parts(h):
        return min(4, size(h, 1))

    def shifts(h, c):
        n = size(h, 1)
        order = sorted(range(n), key=lambda d: (-near(d, n), d))
        return order[c * n // parts(h) : (c + 1) * n // parts(h)]

    def term(h, shift, dest):
        q = lax.rem(place(h, 1) + shift, size(h, 1))
        return wgt_s[(*cell(h, q, dest), h)]

    def reduce_depth(h, c, sign):
        n = size(h, 2)
        return n // 2 if (c % 2 == 0) == (sign > 0) else n // 2 - 1

    def reduce_round(j):
        for c in range(4):
            for h in range(2):
                if c >= parts(h):
                    continue
                n = size(h, 2)
                part = pl.ds(0, size(h, 1) // parts(h))
                for i, sign in enumerate((1, -1)):
                    depth = reduce_depth(h, c, sign)
                    k = j - (n // 2 - depth)
                    if k < 1 or k > depth:
                        continue
                    dest = lax.rem(place(h, 2) + sign * (depth - k + 1) + n, n)
                    if k > 1:
                        hops[h, c, sign, k - 1].wait_recv()
                    for j_at, shift in enumerate(shifts(h, c)):
                        value = term(h, shift, dest)
                        if k > 1:
                            value = value + rs_r[h, c, i, k - 2, j_at].astype(F32)
                        rs_s[h, c, i, k - 1, j_at] = value.astype(BF16)
                    hops[h, c, sign, k] = send(
                        rs_s.at[h, c, i, k - 1, part],
                        rs_r.at[h, c, i, k - 1, part],
                        a2_rs.at[h, 2 * c + (k - 1) // 2, i * (n // 2 - 1) + (k - 1) % 2],
                        along(h, 2, sign),
                    )

    def reduce_finish(chunks):
        for c in chunks:
            for h in range(2):
                if c >= parts(h):
                    continue
                for i, sign in enumerate((1, -1)):
                    if reduce_depth(h, c, sign):
                        hops[h, c, sign, reduce_depth(h, c, sign)].wait_recv()
                for j_at, shift in enumerate(shifts(h, c)):
                    value = term(h, shift, place(h, 2))
                    for i, sign in enumerate((1, -1)):
                        if reduce_depth(h, c, sign):
                            value = value + rs_r[h, c, i, reduce_depth(h, c, sign) - 1, j_at].astype(F32)
                    if shift == 0:
                        wgt_s[z, y, h] = value
                        continue
                    q_s[h, shift] = value.astype(BF16)
                    last[h, shift] = send(
                        q_s.at[h, shift], q_r.at[h, shift], r2_rs.at[h, shift - 1], along(h, 1, shift)
                    )

    def reduce_end():
        for h in range(2):
            value = wgt_s[z, y, h]
            for d in range(1, size(h, 1)):
                last[h, d].wait_recv()
                value = value + q_r[h, d].astype(F32)
            wg_ref[h] = value

    for r in range(5, rounds - 1):
        gather_round(r)
    reduce_round(1)
    gather_round(rounds - 1)

    def product_step(i, carry):
        columns = pl.ds(pl.multiple_of(i * block_cols, 128), block_cols)
        part = jnp.dot(
            og_s[:, columns], wt_s[i].reshape(block_cols, width), preferred_element_type=F32
        )
        ag_s[...] = ag_s[...] + part
        return carry

    ag_s[...] = jnp.zeros_like(ag_s)
    lax.fori_loop(0, nz, product_step, 0)
    reduce_round(2)

    def pre_step(i, carry):
        gain_sum, bias_sum = carry
        here = pl.ds(pl.multiple_of(i * chunk, 8), chunk)
        normed = conv_s[here, :]
        pre = normed * gain_ref[...] + bias_ref[...]
        gate = jax.nn.sigmoid(pre)
        pre_grad = ag_s[here, :] * gate * (1.0 + pre * (1.0 - gate))
        gain_sum = gain_sum + jnp.sum((pre_grad * normed).reshape(chunk // 8, 8, width), axis=0)
        bias_sum = bias_sum + jnp.sum(pre_grad.reshape(chunk // 8, 8, width), axis=0)
        normed_grad = pre_grad * gain_ref[...]
        ag_s[here, :] = normed_grad
        s1_s[here, :] = fold(normed_grad)
        s2_s[here, :] = fold(normed_grad * normed)
        return gain_sum, bias_sum

    none = jnp.zeros((8, width), F32)
    gain_sum, bias_sum = lax.fori_loop(0, steps, pre_step, (none, none))
    gain_row = jnp.sum(gain_sum, axis=0, keepdims=True)
    bias_row = jnp.sum(bias_sum, axis=0, keepdims=True)
    sums = row_sums(1)
    reduce_round(3)
    total = gathered_sums(1, sums)
    b1_s[...] = down_rows(total[0:1])
    b2_s[...] = down_rows(total[1:2])

    def conv_grad_step(i, carry):
        base = pl.multiple_of(i * chunk, 8)
        here = pl.ds(base, chunk)
        value = wide(ib_s[here, :]) * (
            ag_s[here, :] - wide(b1_s[here, :]) - conv_s[here, :] * wide(b2_s[here, :])
        )
        cgpad[pl.ds(pl.multiple_of(base + EDGE, 8), chunk), :] = value
        return carry

    lax.fori_loop(0, steps, conv_grad_step, 0)
    back = [
        send(cgpad.at[pl.ds(rows, EDGE)], cg_recv.at[0], halo_rs.at[2], right_dev),
        send(cgpad.at[pl.ds(EDGE, EDGE)], cg_recv.at[1], halo_rs.at[3], left_dev),
    ]

    tacc[...] = jnp.zeros_like(tacc)

    def tap_step(i, carry):
        base = i * chunk
        value = cgpad[pl.ds(base + EDGE, chunk), :]
        for k in range(span):
            term = value * mpad[pl.ds(base + k + 1, chunk), :]
            tacc[k] = tacc[k] + jnp.sum(term.reshape(chunk // 8, 8, width), axis=0)
        return carry

    for i in range(steps):
        tap_step(i, 0)
    own_small = jnp.concatenate(
        [jnp.sum(tacc[...], axis=1), gain_row, bias_row, jnp.zeros((small_ref.shape[0] - span - 2, width), F32)],
        axis=0,
    )
    small_ref[...] = own_small

    def small_send(phase):
        copies = {}
        for h in range(2):
            ar_s[phase - 1, h] = small_ref[:, h * lanes : (h + 1) * lanes].astype(BF16)
        todo = [(-near(d, size(h, phase)), d, h) for h in range(2) for d in range(1, size(h, phase))]
        for _, d, h in sorted(todo):
            copies[h, d] = send(
                ar_s.at[phase - 1, h],
                ar_r.at[phase - 1, h, d],
                ar_rs.at[phase - 1, h, d - 1],
                along(h, phase, d),
            )
        return copies

    def small_add(phase, copies):
        for h in range(2):
            value = ar_s[phase - 1, h].astype(F32)
            for d in range(1, size(h, phase)):
                copies[h, d].wait_recv()
                value = value + ar_r[phase - 1, h, d].astype(F32)
            small_ref[:, h * lanes : (h + 1) * lanes] = value

    small_1 = small_send(1)
    reduce_round(4)

    back[0].wait_recv()
    back[1].wait_recv()
    cgpad[:EDGE] = jnp.where(s == 0, 0.0, cg_recv[0])
    cgpad[EDGE + rows :] = jnp.where(s == count - 1, 0.0, cg_recv[1])

    def mixed_step(i, carry):
        base = i * chunk
        total = jnp.zeros((chunk, width), F32)
        for k in range(span):
            total = total + taps_ref[k : k + 1, :] * cgpad[pl.ds(base + span - k, chunk), :]
        ag_s[pl.ds(base, chunk), :] = total
        return carry

    for i in range(steps):
        mixed_step(i, 0)
    reduce_finish((0, 1, 2))
    small_add(1, small_1)
    small_2 = small_send(2)
    reduce_finish((3,))
    scaled = ag_s[...] * sig_s[...]
    v_s[...] = scaled.astype(BF16)
    g_s[...] = (scaled * vf_s[...] * (1.0 - sig_s[...])).astype(BF16)
    store_v = pltpu.make_async_copy(v_s, vg_hbm, local_sem.at[0])
    store_g = pltpu.make_async_copy(g_s, gg_hbm, local_sem.at[1])
    store_v.start()
    store_g.start()
    reduce_end()
    small_add(2, small_2)
    store_v.wait()
    store_g.wait()
    for copy in pending[-slots:]:
        copy.wait_send()


def finish(span, vg_ref, gg_ref, small_ref, wg_ref, vg_out, gg_out, tap_out, gain_out, bias_out, wg_out):
    vg_out[...] = vg_ref[...]
    gg_out[...] = gg_ref[...]
    wg_out[...] = wg_ref[...]
    tap_out[...] = small_ref[:span]
    gain_out[...] = small_ref[span : span + 1]
    bias_out[...] = small_ref[span + 1 : span + 2]


def on_device(sizes, value_in, gate_in, taps, norm_gain, norm_bias, proj_weight, out_grad):
    nz, ny, nt = sizes
    rows, width = value_in.shape
    span = taps.shape[0]
    n_col = proj_weight.shape[1]
    quarter = n_col // 2
    columns = out_grad.shape[1]
    lanes = width // 2
    chunk = next(c for c in (72, 24, 8) if rows % c == 0)
    padded_rows = (rows + 127) // 128 * 128
    small_rows = (span + 2 + 7) // 8 * 8
    n_max = max(nz, ny)
    n_half = n_max // 2
    dma = pltpu.SemaphoreType.DMA
    vmem = pl.BlockSpec(memory_space=pltpu.VMEM)
    hbm = pl.BlockSpec(memory_space=pltpu.HBM)
    cfg = (nz, ny, nt, rows, width, span, chunk)
    vg, gg, small, wg = pl.pallas_call(
        functools.partial(kernel, cfg),
        out_shape=(
            jax.ShapeDtypeStruct((rows, width), BF16),
            jax.ShapeDtypeStruct((rows, width), BF16),
            jax.ShapeDtypeStruct((small_rows, width), F32),
            jax.ShapeDtypeStruct((2, quarter, width), F32),
        ),
        in_specs=[hbm] * 7,
        out_specs=(hbm, hbm, vmem, vmem),
        scratch_shapes=[
            pltpu.VMEM((rows, width), BF16),
            pltpu.VMEM((rows, width), BF16),
            pltpu.VMEM((rows, columns), BF16),
            pltpu.VMEM((span, width), F32),
            pltpu.VMEM((1, width), F32),
            pltpu.VMEM((1, width), F32),
            pltpu.VMEM((rows, width), F32),
            pltpu.VMEM((rows, width), F32),
            pltpu.VMEM((rows + 2 * EDGE, width), F32),
            pltpu.VMEM((rows, width), F32),
            pltpu.VMEM((padded_rows, lanes), F32),
            pltpu.VMEM((padded_rows, lanes), F32),
            pltpu.VMEM((padded_rows, lanes), F32),
            pltpu.VMEM((padded_rows, lanes), F32),
            pltpu.VMEM((padded_rows, lanes), F32),
            pltpu.VMEM((rows, width), F32),
            pltpu.VMEM((rows, width), BF16),
            pltpu.VMEM((rows, width), F32),
            pltpu.VMEM((rows + 2 * EDGE, width), F32),
            pltpu.VMEM((span, 8, width), F32),
            pltpu.VMEM((2, EDGE, width), BF16),
            pltpu.VMEM((2, EDGE, width), BF16),
            pltpu.VMEM((2, EDGE, width), F32),
            pltpu.VMEM((2, 2, padded_rows), F32),
            pltpu.VMEM((2, nt, 2, padded_rows), F32),
            pltpu.VMEM((nz, ny, 2, quarter, width), BF16),
            pltpu.VMEM((nz, ny, 2, quarter, width), F32),
            pltpu.VMEM((2, 4, 2, n_half, max(1, n_max // 4), quarter, width), BF16),
            pltpu.VMEM((2, 4, 2, n_half, max(1, n_max // 4), quarter, width), BF16),
            pltpu.VMEM((2, n_max, quarter, width), BF16),
            pltpu.VMEM((2, n_max, quarter, width), BF16),
            pltpu.VMEM((2, 2, small_rows, lanes), BF16),
            pltpu.VMEM((2, 2, n_max, small_rows, lanes), BF16),
            dma((7,)),
            dma((40,)),
            dma((4,)),
            dma((2, nt - 1)),
            dma((2, n_max - 1)),
            dma((2, n_max, n_max - 1)),
            dma((2, n_max - 1)),
            dma((2, 2, n_max - 1)),
        ],
        compiler_params=pltpu.CompilerParams(
            collective_id=0, has_side_effects=True, vmem_limit_bytes=60 * 1024 * 1024
        ),
        name="step",
    )(
        value_in,
        gate_in,
        taps,
        norm_gain[None, :],
        norm_bias[None, :],
        proj_weight.T.reshape(2, quarter, width),
        out_grad,
    )
    vg, gg, tap, gain, bias, wg = pl.pallas_call(
        functools.partial(finish, span),
        out_shape=(
            jax.ShapeDtypeStruct((rows, width), BF16),
            jax.ShapeDtypeStruct((rows, width), BF16),
            jax.ShapeDtypeStruct((span, width), F32),
            jax.ShapeDtypeStruct((1, width), F32),
            jax.ShapeDtypeStruct((1, width), F32),
            jax.ShapeDtypeStruct((2, quarter, width), F32),
        ),
        in_specs=[vmem] * 4,
        out_specs=(vmem,) * 6,
        compiler_params=pltpu.CompilerParams(vmem_limit_bytes=60 * 1024 * 1024),
        name="finish",
    )(vg, gg, small, wg)
    return (vg, gg, tap, gain[0], bias[0], jnp.transpose(wg.reshape(n_col, width)))


def solution(mesh):
    tp = mesh.shape["tp"]
    ny = 8 if mesh.shape["sp"] % 8 == 0 else 2
    nz = mesh.shape["sp"] // ny
    finer = Mesh(mesh.devices.reshape(nz, ny, tp), (*SP, "tp"))
    in_specs = (P(SP, "tp"), P(SP, "tp"), P(None, "tp"), P("tp"), P("tp"), P("tp", SP), P(SP, None))
    out_specs = (P(SP, "tp"), P(SP, "tp"), P(None, "tp"), P("tp"), P("tp"), P("tp", SP))
    return jax.shard_map(
        functools.partial(on_device, (nz, ny, tp)),
        mesh=finer,
        in_specs=in_specs,
        out_specs=out_specs,
        check_vma=False,
    )
```
